32 devices in a mesh: sp: 16 (over z, y, x), tp: 2 (over core).
Axes of the slice: x: 2, y: 2, z: 4, core: 2. Of those that a mesh axis runs over, the one named last changes fastest.
Arguments:
- stream: bfloat16 [7168, 2048], P('sp'), may hold values from -6 to 6
- norm_gain: float32 [2, 2048], replicated, may hold values from 0.1 to 1.9
- value_weight: bfloat16 [2, 2048, 512], P(None, None, 'tp'), may hold values from -0.125 to 0.125
- gate_weight: bfloat16 [2, 2048, 512], P(None, None, 'tp'), may hold values from -0.125 to 0.125
- conv_taps: bfloat16 [2, 512, 512], P(None, None, 'tp'), may hold values from -0.25 to 0.25
- conv_bias: float32 [2, 512], P(None, 'tp'), may hold values from -3 to 3
- channel_gain: float32 [2, 512], replicated, may hold values from 0.1 to 1.9
- channel_shift: float32 [2, 512], replicated, may hold values from -3 to 3
- out_weight: bfloat16 [2, 512, 2048], replicated, may hold values from -0.25 to 0.25
Outputs:
- result: bfloat16 [7168, 2048], P('sp')
The draws below stay inside these ranges and needn't reach their ends.
All inputs are finite; a program needn't handle non-finite values.
Results may differ from the reference program's by a relative error of at most 0.0075.
Values may be sent and summed in bfloat16 or wider, within the bound.
A program may use at most 64 MiB of HBM per device.

```python
import jax
import jax.numpy as jnp
from jax import lax

D = 2048
CH = 512
KW = 512
LAYERS = 2
TOKENS = 7168


def block_scale(key, shape, pieces, smallest, high):
    loudness, own = 1.0, jax.random.fold_in(key, 6)
    for dim, parts in pieces:
        steps = jnp.exp(jax.random.uniform(jax.random.fold_in(own, dim), (parts,), jnp.float32, smallest / len(pieces), high / len(pieces)))
        loudness = loudness * jnp.repeat(steps, shape[dim] // parts).reshape([-1 if axis == dim else 1 for axis in range(len(shape))])
    return loudness


def scatter_about(stream_key, dims, scale, most, split=(), held_as=jnp.bfloat16):
    array = scale * jax.random.normal(stream_key, dims, jnp.float32)
    if split:
        array = array * block_scale(stream_key, dims, split, -0.22, 0.18)
    return jnp.clip(array, -most, most).astype(held_as)


def setup_inputs(seed: int = 0) -> dict:
    key_list = jax.random.split(jax.random.key(seed), 10)
    stream = scatter_about(key_list[0], (TOKENS, D), 1.0, 6.0, ((0, 16),))
    norm_gain = jnp.clip(1.0 + 0.18 * jax.random.normal(key_list[1], (LAYERS, D), jnp.float32), 0.1, 1.9)
    value_weight = scatter_about(key_list[2], (LAYERS, D, CH), D ** -0.5, 0.125, ((2, 2),))
    gate_weight = scatter_about(key_list[3], (LAYERS, D, CH), D ** -0.5, 0.125, ((2, 2),))
    conv_taps = scatter_about(key_list[4], (LAYERS, KW, CH), KW ** -0.5, 0.25, ((2, 2),))
    conv_bias = scatter_about(key_list[5], (LAYERS, CH), 0.5, 3.0, ((1, 2),), jnp.float32)
    channel_gain = jnp.clip(1.0 + 0.18 * jax.random.normal(key_list[6], (LAYERS, CH), jnp.float32), 0.1, 1.9)
    channel_shift = scatter_about(key_list[7], (LAYERS, CH), 0.5, 3.0, (), jnp.float32)
    out_weight = scatter_about(key_list[8], (LAYERS, CH, D), CH ** -0.5, 0.25)
    return dict(stream=stream, norm_gain=norm_gain, value_weight=value_weight, gate_weight=gate_weight, conv_taps=conv_taps, conv_bias=conv_bias, channel_gain=channel_gain, channel_shift=channel_shift, out_weight=out_weight)


def rms_normed(stream, gain):
    values = stream.astype(jnp.float32)
    scale = lax.rsqrt(lax.optimization_barrier(jnp.mean(values * values, axis=-1, keepdims=True)) + 1e-06)
    return (values * scale * gain[None, :]).astype(jnp.bfloat16)

def channel_mix(conv, gain, shift):
    values = conv.astype(jnp.float32)
    center = lax.optimization_barrier(jnp.mean(values, axis=-1, keepdims=True))
    spread = lax.optimization_barrier(jnp.mean(jnp.square(values - center), axis=-1, keepdims=True))
    normed = (values - center) * lax.rsqrt(spread + 1e-05) * gain[None, :] + shift[None, :]
    return jax.nn.silu(normed).astype(jnp.bfloat16)

def causal_conv(gated, taps):
    length = gated.shape[0]
    span = taps.shape[0]
    padded_len = 1 << (length + span - 2).bit_length()
    signal = jnp.fft.rfft(gated.astype(jnp.float32), n=padded_len, axis=0)
    kernel = jnp.fft.rfft(taps.astype(jnp.float32)[::-1], n=padded_len, axis=0)
    return jnp.fft.irfft(signal * kernel, n=padded_len, axis=0)[:length]

def reference(stream, norm_gain, value_weight, gate_weight, conv_taps, conv_bias, channel_gain, channel_shift, out_weight):
    state = stream
    for layer in range(LAYERS):
        normed = rms_normed(state, norm_gain[layer])
        values = jnp.dot(normed, value_weight[layer], preferred_element_type=jnp.float32)
        gates = jnp.dot(normed, gate_weight[layer], preferred_element_type=jnp.float32)
        gated = (values * jax.nn.sigmoid(gates)).astype(jnp.bfloat16)
        conv = causal_conv(gated, conv_taps[layer])
        conv = (conv + conv_bias[layer][None, :]).astype(jnp.bfloat16)
        mixed = channel_mix(conv, channel_gain[layer], channel_shift[layer])
        update = jnp.dot(mixed, out_weight[layer], preferred_element_type=jnp.float32)
        state = (state.astype(jnp.float32) + update).astype(jnp.bfloat16)
    return state
```

```python
import functools

import jax
import jax.numpy as jnp
import numpy as np
from jax import lax
from jax.experimental import pallas as pl
from jax.experimental.pallas import tpu as pltpu
from jax.sharding import PartitionSpec as P

BLOCK = 128
MESH = pl.DeviceIdType.MESH


def dft_matrices(block):
    span = 2 * block
    angle = 2 * np.pi / span * np.outer(np.arange(block) + 0.5, np.arange(span))
    forward = np.concatenate([np.cos(angle), -np.sin(angle)], axis=0)
    of_taps = forward[:, block - 1 :: -1]
    inverse = forward[:, block:].T / block
    return [jnp.asarray(m, jnp.bfloat16) for m in (forward, of_taps, inverse)]


class Plan:
    def __init__(self, tokens, width, reach, n_sp):
        self.tokens, self.n_sp = tokens, n_sp
        self.parts = reach // BLOCK
        self.outs = -(-tokens // BLOCK)
        self.rows = (self.parts + self.outs) * BLOCK
        self.own = self.rows - tokens
        low = self.own - reach
        self.chunks = []
        for p in reversed(range(self.outs)):
            start = (self.parts + p) * BLOCK
            self.chunks.append((max(start, self.own), start + BLOCK))
        self.pieces = []
        for c, (a, b) in enumerate(self.chunks):
            for hop in range(1, min(-(-reach // tokens), n_sp - 1) + 1):
                first, end = max(a, low + hop * tokens) - hop * tokens, b - hop * tokens
                while first < end:
                    cut = max(first, (end - 1) // BLOCK * BLOCK if end <= self.outs * BLOCK else first)
                    when = c if hop == 1 else max(c, self.outs - 2)
                    self.pieces.append((when, hop, cut + hop * tokens, cut, end - cut))
                    end = cut
        self.pieces.sort(key=lambda piece: piece[:2])


def scoped(fn):
    def named(*args):
        label = "_".join(str(a) for a in args if isinstance(a, int))
        with jax.named_scope(f"{fn.__name__}#{label}"):
            return fn(*args)

    return named


def kernel(
    plan, layers, stream, gain, wv, wg, taps, bias, cgain, cshift, wo, fwd, oft, inv, x_v,
    gain_v, w_v, taps_v, bias_v, cgain_v, cshift_v, wo_v, fwd_v, oft_v, inv_v,
    gated, gained, spectra, kernels, freq, conv, peer, load_sem, send_sem, recv_sem, swap_send, swap_recv,
):
    sp, tp = lax.axis_index("sp"), lax.axis_index("tp")
    half = wv.shape[2]
    width = x_v.shape[1]
    mine = pl.ds(pl.multiple_of(tp * half, half), half)
    other = pl.ds(pl.multiple_of((1 - tp) * half, half), half)
    first, second = pl.ds(0, half), pl.ds(half, half)
    loads = {}

    def load(name, source, target):
        copy = pltpu.make_async_copy(source, target, load_sem.at[len(loads)])
        loads[name] = copy
        copy.start()

    waited = set()

    def need(*names):
        for name in names:
            if name not in waited:
                waited.add(name)
                loads[name].wait()

    def own_rows(c):
        a, b = plan.chunks[c]
        return pl.ds(a - plan.own, b - a)

    load("gain", gain, gain_v)
    load(("x", 0), stream.at[own_rows(0)], x_v.at[own_rows(0)])
    load(("wv", 0), wv.at[0], w_v.at[0, :, first])
    load(("wg", 0), wg.at[0], w_v.at[0, :, second])
    for c in range(1, plan.outs):
        load(("x", c), stream.at[own_rows(c)], x_v.at[own_rows(c)])
    load("oft", oft, oft_v)
    load("taps", taps, taps_v)
    load("fwd", fwd, fwd_v)
    load("inv", inv, inv_v)
    load("bias", bias, bias_v)
    load("cgain0", cgain.at[:, mine], cgain_v.at[:, first])
    load("cgain1", cgain.at[:, other], cgain_v.at[:, second])
    load("cshift0", cshift.at[:, mine], cshift_v.at[:, first])
    load("cshift1", cshift.at[:, other], cshift_v.at[:, second])
    for l in range(layers):
        if l:
            load(("wv", l), wv.at[l], w_v.at[l, :, first])
            load(("wg", l), wg.at[l], w_v.at[l, :, second])
        load(("wo0", l), wo.at[l, mine], wo_v.at[l, first])
        load(("wo1", l), wo.at[l, other], wo_v.at[l, second])

    for l in range(layers):
        gated[l, : plan.own] = jnp.zeros((plan.own, half), jnp.bfloat16)

    hops = sorted({piece[1] for piece in plan.pieces})
    barrier = pltpu.get_barrier_semaphore()
    pl.semaphore_signal(barrier, inc=1, device_id={"tp": 1 - tp}, device_id_type=MESH)
    for hop in hops:
        @pl.when(sp >= hop)
        def _():
            pl.semaphore_signal(barrier, inc=1, device_id={"sp": sp - hop}, device_id_type=MESH)

    def piece_copy(l, i):
        _, hop, source, target, count = plan.pieces[i]
        return pltpu.make_async_remote_copy(
            src_ref=gated.at[l, pl.ds(source, count)],
            dst_ref=gated.at[l, pl.ds(target, count)],
            send_sem=send_sem.at[l, i],
            recv_sem=recv_sem.at[l, i],
            device_id={"sp": sp + hop},
            device_id_type=MESH,
        )

    def swap_copy(l, c):
        return pltpu.make_async_remote_copy(
            src_ref=conv.at[l, own_rows(c)],
            dst_ref=peer.at[l, own_rows(c)],
            send_sem=swap_send.at[l, c],
            recv_sem=swap_recv.at[l, c],
            device_id={"tp": 1 - tp},
            device_id_type=MESH,
        )

    @scoped
    def gate(l, c, squares=None):
        rows = own_rows(c)
        need("gain", ("wv", l), ("wg", l))
        if squares is None:
            need(("x", c))
            squares = 0.0
            step = width // 4
            for k in range(0, width, step):
                x = x_v[rows, k : k + step].astype(jnp.float32)
                squares = squares + jnp.sum(x * x, axis=-1, keepdims=True)
                gained[rows, k : k + step] = (x * gain_v[l : l + 1, k : k + step]).astype(jnp.bfloat16)
        both = jnp.dot(gained[rows, :], w_v[l], preferred_element_type=jnp.float32)
        both = both * lax.rsqrt(squares / width + 1e-06)
        a, b = plan.chunks[c]
        gated[l, a:b, :] = (both[:, :half] * jax.nn.sigmoid(both[:, half:])).astype(jnp.bfloat16)

    @scoped
    def send(l, c):
        for i, piece in enumerate(plan.pieces):
            if piece[0] == c:
                @pl.when(sp + piece[1] < plan.n_sp)
                def _():
                    piece_copy(l, i).start()

    @scoped
    def transform_taps(l):
        need("oft", "taps")
        for j in range(plan.parts):
            first = (plan.parts - 1 - j) * BLOCK
            kernels[l, j] = jnp.dot(
                oft_v[...], taps_v[l, first : first + BLOCK, :], preferred_element_type=jnp.float32
            )

    arrived = set()

    def await_pieces(l, w):
        first, last = w * BLOCK, (w + 2) * BLOCK
        for i, (_, hop, _, target, count) in enumerate(plan.pieces):
            if (l, i) not in arrived and target < last and target + count > first:
                arrived.add((l, i))
                with jax.named_scope(f"recv{i}"):
                    @pl.when(sp >= hop)
                    def _():
                        piece_copy(l, i).wait_recv()

    @scoped
    def spectrum(l, w):
        need("fwd")
        first, last = w * BLOCK, (w + 2) * BLOCK
        spectra[l, w] = jnp.dot(fwd_v[...], gated[l, first:last, :], preferred_element_type=jnp.float32)

    @scoped
    def convolve(l, c):
        p = plan.outs - 1 - c
        tile = 16
        for k in range(0, BLOCK, tile):
            low, high = slice(k, k + tile), slice(BLOCK + k, BLOCK + k + tile)
            real = imag = None
            for j in range(plan.parts):
                w = plan.parts - 1 + p - j
                xr, xi = spectra[l, w, low, :], spectra[l, w, high, :]
                hr, hi = kernels[l, j, low, :], kernels[l, j, high, :]
                r, i = xr * hr - xi * hi, xr * hi + xi * hr
                real, imag = (r, i) if real is None else (real + r, imag + i)
            freq[low, :] = real.astype(jnp.bfloat16)
            freq[high, :] = imag.astype(jnp.bfloat16)
        a, b = plan.chunks[c]
        result = jnp.dot(inv_v[BLOCK - (b - a) :, :], freq[...], preferred_element_type=jnp.float32)
        conv[l, own_rows(c), :] = (result + bias_v[l : l + 1, :]).astype(jnp.bfloat16)
        swap_copy(l, c).start()

    @scoped
    def finish(l, c):
        rows = own_rows(c)
        last = l == layers - 1
        with jax.named_scope("swapwait"):
            swap_copy(l, c).wait()
        need("cgain0", "cgain1", "cshift0", "cshift1", ("wo0", l), ("wo1", l))
        if not last:
            need(("wv", l + 1), ("wg", l + 1))
        values = jnp.concatenate([conv[l, rows, :], peer[l, rows, :]], axis=-1).astype(jnp.float32)
        center = jnp.mean(values, axis=-1, keepdims=True)
        values = values - center
        spread = jnp.mean(values * values, axis=-1, keepdims=True)
        normed = values * lax.rsqrt(spread + 1e-05) * cgain_v[l : l + 1, :] + cshift_v[l : l + 1, :]
        mixed = (normed * jax.nn.sigmoid(normed)).astype(jnp.bfloat16)
        step = width // 4
        squares = 0.0
        for n in range(0, width, step):
            update = jnp.dot(mixed, wo_v[l, :, n : n + step], preferred_element_type=jnp.float32)
            new = (x_v[rows, n : n + step].astype(jnp.float32) + update).astype(jnp.bfloat16)
            x_v[rows, n : n + step] = new
            if not last:
                x = new.astype(jnp.float32)
                squares = squares + jnp.sum(x * x, axis=-1, keepdims=True)
                gained[rows, n : n + step] = (x * gain_v[l + 1 : l + 2, n : n + step]).astype(jnp.bfloat16)
        if not last:
            gate(l + 1, c, squares)

    for c in range(plan.outs):
        gate(0, c)
        if c == 0:
            with jax.named_scope("barrier"):
                pl.semaphore_wait(barrier, 1 + jnp.minimum(plan.n_sp - 1 - sp, len(hops)))
        send(0, c)
    need("inv", "bias")
    for l in range(layers):
        transform_taps(l)
    for l in range(layers):
        last = l == layers - 1
        windows = plan.parts + plan.outs - 1
        done = windows

        def after(c):
            finish(l, c)
            if not last:
                send(l + 1, c)

        finished = 0
        for c in range(plan.outs):
            fresh = list(range(done - 1, plan.outs - 2 - c, -1))
            done = plan.outs - 1 - c
            own = [w for w in fresh if w * BLOCK >= plan.own]
            for w in own:
                spectrum(l, w)
            for w in fresh:
                await_pieces(l, w)
            for w in fresh:
                if w not in own:
                    spectrum(l, w)
            convolve(l, c)
            due = c
            while finished < due:
                after(finished)
                finished += 1
        while finished < plan.outs:
            after(finished)
            finished += 1

    for l in range(layers):
        for i, piece in enumerate(plan.pieces):
            @pl.when(sp + piece[1] < plan.n_sp)
            def _():
                piece_copy(l, i).wait_send()


def per_device(stream, norm_gain, value_weight, gate_weight, conv_taps, conv_bias, channel_gain, channel_shift, out_weight):
    tokens, width = stream.shape
    layers, reach, half = conv_taps.shape
    plan = Plan(tokens, width, reach, lax.axis_size("sp"))
    mats = dft_matrices(BLOCK)
    n_pieces = len(plan.pieces)
    bf16, f32, dma = jnp.bfloat16, jnp.float32, pltpu.SemaphoreType.DMA
    windows = plan.parts + plan.outs - 1
    return pl.pallas_call(
        functools.partial(kernel, plan, layers),
        out_shape=pltpu.VMEM(stream.shape, stream.dtype),
        in_specs=[pl.BlockSpec(memory_space=pltpu.HBM)] * 12,
        out_specs=pl.BlockSpec(memory_space=pltpu.VMEM),
        scratch_shapes=[
            pltpu.VMEM(norm_gain.shape, f32),
            pltpu.VMEM((layers, width, 2 * half), bf16),
            pltpu.VMEM(conv_taps.shape, bf16),
            pltpu.VMEM(conv_bias.shape, f32),
            pltpu.VMEM(channel_gain.shape, f32),
            pltpu.VMEM(channel_shift.shape, f32),
            pltpu.VMEM(out_weight.shape, bf16),
            *[pltpu.VMEM(m.shape, bf16) for m in mats],
            pltpu.VMEM((layers, plan.rows, half), bf16),
            pltpu.VMEM((tokens, width), bf16),
            pltpu.VMEM((layers, windows, 2 * BLOCK, half), f32),
            pltpu.VMEM((layers, plan.parts, 2 * BLOCK, half), f32),
            pltpu.VMEM((2 * BLOCK, half), bf16),
            pltpu.VMEM((layers, tokens, half), bf16),
            pltpu.VMEM((layers, tokens, half), bf16),
            dma((10 + plan.outs + 4 * layers,)),
            dma((layers, n_pieces)),
            dma((layers, n_pieces)),
            dma((layers, plan.outs)),
            dma((layers, plan.outs)),
        ],
        compiler_params=pltpu.CompilerParams(
            collective_id=0, has_side_effects=True, vmem_limit_bytes=60000 * 1024
        ),
    )(stream, norm_gain, value_weight, gate_weight, conv_taps, conv_bias, channel_gain, channel_shift, out_weight, *mats)


def solution(mesh):
    return jax.shard_map(
        per_device,
        mesh=mesh,
        in_specs=(
            P("sp", None),
            P(),
            P(None, None, "tp"),
            P(None, None, "tp"),
            P(None, None, "tp"),
            P(None, "tp"),
            P(),
            P(),
            P(),
        ),
        out_specs=P("sp", None),
        check_vma=False,
    )
```

```python
import functools

import jax
import jax.numpy as jnp
import numpy as np
from jax import lax
from jax.experimental import pallas as pl
from jax.experimental.pallas import tpu as pltpu
from jax.sharding import PartitionSpec as P

BLOCK = 128
MESH = pl.DeviceIdType.MESH


def dft_matrices(block):
    span = 2 * block
    angle = 2 * np.pi / span * np.outer(np.arange(block) + 0.5, np.arange(span))
    forward = np.concatenate([np.cos(angle), -np.sin(angle)], axis=0)
    of_taps = forward[:, block - 1 :: -1]
    inverse = forward[:, block:].T / block
    of_taps = np.concatenate([of_taps, np.zeros_like(of_taps)], axis=1)
    return jnp.asarray(np.concatenate([forward, inverse, of_taps]), jnp.bfloat16)


class Plan:
    def __init__(self, tokens, width, reach, n_sp):
        self.tokens, self.n_sp = tokens, n_sp
        self.parts = reach // BLOCK
        self.outs = -(-tokens // BLOCK)
        self.rows = (self.parts + self.outs) * BLOCK
        self.own = self.rows - tokens
        low = self.own - reach
        self.chunks = []
        for p in reversed(range(self.outs)):
            start = (self.parts + p) * BLOCK
            self.chunks.append((max(start, self.own), start + BLOCK))
        self.groups = [[c] for c in range(self.outs - 2)] + [list(range(max(self.outs - 2, 0), self.outs))]
        self.pieces = []
        for c, (a, b) in enumerate(self.chunks):
            for hop in range(1, min(-(-reach // tokens), n_sp - 1) + 1):
                first, end = max(a, low + hop * tokens) - hop * tokens, b - hop * tokens
                while first < end:
                    cut = max(first, (end - 1) // BLOCK * BLOCK if end <= self.outs * BLOCK else first)
                    when = c if hop == 1 else max(self.outs - 3, 0)
                    self.pieces.append((when, hop, cut + hop * tokens, cut, end - cut))
                    end = cut
        self.pieces.sort(key=lambda piece: piece[:2])
        self.needs = []
        for _, _, _, target, count in self.pieces:
            for g, group in enumerate(self.groups):
                if target + count > (self.outs - 1 - group[-1]) * BLOCK:
                    self.needs.append(g)
                    break


def scoped(fn):
    def named(*args):
        label = "_".join(str(a) for a in args if isinstance(a, (int, list)))
        with jax.named_scope(f"{fn.__name__}#{label}"):
            return fn(*args)

    return named


def kernel(
    plan, layers, stream, gain, wv, wg, taps, bias, cgain, cshift, wo, mats, x_v, mixed_v, wo_last,
    gain_v, w_v, taps_v, bias_v, cgain_v, cshift_v, wo_v, mats_v,
    gated, gained, spectra, kernels, freq, conv, peer, load_sem, send_sem, recv_sem, swap_send, swap_recv,
):
    sp, tp = lax.axis_index("sp"), lax.axis_index("tp")
    half = wv.shape[2]
    width = x_v.shape[1]
    mine = pl.ds(pl.multiple_of(tp * half, half), half)
    other = pl.ds(pl.multiple_of((1 - tp) * half, half), half)
    first, second = pl.ds(0, half), pl.ds(half, half)
    loads = {}
    waited = set()

    def load(key, whole, *parts):
        sem = load_sem.at[len(loads)]
        loads[key] = pltpu.make_async_copy(whole, whole, sem)
        for source, target in parts:
            pltpu.make_async_copy(source, target, sem).start()

    def need(*keys):
        for key in keys:
            if key not in waited:
                waited.add(key)
                loads[key].wait()

    def own_rows(c):
        a, b = plan.chunks[c]
        return pl.ds(a - plan.own, b - a)

    def load_rows(key, a, b):
        rows = pl.ds(a, b - a)
        load(key, x_v.at[rows], (stream.at[rows], x_v.at[rows]))

    def load_gate(l):
        load(("gate", l), w_v.at[l], (wv.at[l], w_v.at[l, :, first]), (wg.at[l], w_v.at[l, :, second]))

    def load_halves(key, source, target):
        load(key, target, (source(mine), target.at[first]), (source(other), target.at[second]))

    head = plan.chunks[0][0] - plan.own
    load("gain", gain_v, (gain, gain_v))
    load_rows("x0", head, x_v.shape[0])
    load_gate(0)
    load_rows("x", 0, head)
    load("taps", taps_v, (taps, taps_v))
    load("mats", mats_v, (mats, mats_v))
    load("bias", bias_v, (bias, bias_v))
    load("cgain", cgain_v, (cgain.at[:, mine], cgain_v.at[:, first]), (cgain.at[:, other], cgain_v.at[:, second]))
    load("cshift", cshift_v, (cshift.at[:, mine], cshift_v.at[:, first]), (cshift.at[:, other], cshift_v.at[:, second]))
    for l in range(layers):
        if l:
            load_gate(l)
        load_halves(("out", l), lambda channels: wo.at[l, channels], wo_last if l == layers - 1 else wo_v.at[l])
    fwd_v, inv_v = mats_v.at[: 2 * BLOCK], mats_v.at[2 * BLOCK : 3 * BLOCK]
    oft_v = mats_v.at[3 * BLOCK :, :BLOCK]

    for l in range(layers):
        gated[l, : plan.own] = jnp.zeros((plan.own, half), jnp.bfloat16)

    hops = sorted({piece[1] for piece in plan.pieces})
    barrier = pltpu.get_barrier_semaphore()
    pl.semaphore_signal(barrier, inc=1, device_id={"tp": 1 - tp}, device_id_type=MESH)
    for hop in hops:
        @pl.when(sp >= hop)
        def _():
            pl.semaphore_signal(barrier, inc=1, device_id={"sp": sp - hop}, device_id_type=MESH)

    def piece_copy(l, i):
        _, hop, source, target, count = plan.pieces[i]
        return pltpu.make_async_remote_copy(
            src_ref=gated.at[l, pl.ds(source, count)],
            dst_ref=gated.at[l, pl.ds(target, count)],
            send_sem=send_sem.at[hops.index(hop)],
            recv_sem=recv_sem.at[l, hops.index(hop), plan.needs[i]],
            device_id={"sp": sp + hop},
            device_id_type=MESH,
        )

    group_of = {c: g for g, group in enumerate(plan.groups) for c in group}

    def swap_copy(l, c):
        return pltpu.make_async_remote_copy(
            src_ref=conv.at[l, own_rows(c)],
            dst_ref=peer.at[l, own_rows(c)],
            send_sem=swap_send.at[0],
            recv_sem=swap_recv.at[l, group_of[c]],
            device_id={"tp": 1 - tp},
            device_id_type=MESH,
        )

    def span(group):
        return plan.chunks[group[-1]][0], plan.chunks[group[0]][1]

    def span_rows(group):
        a, b = span(group)
        return pl.ds(a - plan.own, b - a)

    @scoped
    def gate(l, group, squares=None):
        rows = span_rows(group)
        if squares is None:
            need("gain", "x" if group[0] else "x0")
            squares = 0.0
            step = width // 4
            for k in range(0, width, step):
                x = x_v[rows, k : k + step].astype(jnp.float32)
                squares = squares + jnp.sum(x * x, axis=-1, keepdims=True)
                gained[rows, k : k + step] = (x * gain_v[l : l + 1, k : k + step]).astype(jnp.bfloat16)
        need(("gate", l))
        both = jnp.dot(gained[rows, :], w_v[l], preferred_element_type=jnp.float32)
        both = both * lax.rsqrt(squares / width + 1e-06)
        a, b = span(group)
        gated[l, a:b, :] = (both[:, :half] * jax.nn.sigmoid(both[:, half:])).astype(jnp.bfloat16)

    @scoped
    def send(l, c):
        for i, piece in enumerate(plan.pieces):
            if piece[0] == c:
                @pl.when(sp + piece[1] < plan.n_sp)
                def _():
                    piece_copy(l, i).start()

    @scoped
    def transform_taps(l):
        need("taps", "mats")
        for j in range(plan.parts):
            first = (plan.parts - 1 - j) * BLOCK
            kernels[l, j] = jnp.dot(
                oft_v[...], taps_v[l, first : first + BLOCK, :], preferred_element_type=jnp.float32
            )

    def whole(ref, sem):
        return pltpu.make_async_copy(ref, ref, sem)

    def await_group(l, g):
        for h, hop in enumerate(hops):
            spans = [(piece[3], piece[3] + piece[4]) for i, piece in enumerate(plan.pieces) if plan.needs[i] == g and piece[1] == hop]
            if spans:
                low, high = min(a for a, _ in spans), max(b for _, b in spans)
                assert high - low == sum(b - a for a, b in spans)
                with jax.named_scope(f"recv{hop}_{g}"):
                    @pl.when(sp >= hop)
                    def _():
                        whole(gated.at[l, pl.ds(low, high - low)], recv_sem.at[l, h, g]).wait()

    @scoped
    def spectrum(l, w):
        first, last = w * BLOCK, (w + 2) * BLOCK
        spectra[l, w] = jnp.dot(fwd_v[...], gated[l, first:last, :], preferred_element_type=jnp.float32)

    def mix_bins(l, c):
        p = plan.outs - 1 - c
        tile = 16
        for k in range(0, BLOCK, tile):
            low, high = slice(k, k + tile), slice(BLOCK + k, BLOCK + k + tile)
            real = imag = None
            for j in range(plan.parts):
                w = plan.parts - 1 + p - j
                xr, xi = spectra[l, w, low, :], spectra[l, w, high, :]
                hr, hi = kernels[l, j, low, :], kernels[l, j, high, :]
                r, i = xr * hr - xi * hi, xr * hi + xi * hr
                real, imag = (r, i) if real is None else (real + r, imag + i)
            freq[c, low, :] = real.astype(jnp.bfloat16)
            freq[c, high, :] = imag.astype(jnp.bfloat16)

    def invert(l, c):
        a, b = plan.chunks[c]
        result = jnp.dot(inv_v[BLOCK - (b - a) :, :], freq[c], preferred_element_type=jnp.float32)
        conv[l, own_rows(c), :] = (result + bias_v[l : l + 1, :]).astype(jnp.bfloat16)
        swap_copy(l, c).start()

    transformed = set()

    def spectra_for(l, group, own):
        p = plan.outs - 1 - group[-1]
        q = plan.outs - 1 - group[0]
        fresh = [w for w in range(p, q + plan.parts) if (l, w) not in transformed]
        fresh = [w for w in reversed(fresh) if not own or w * BLOCK >= plan.own]
        if not own:
            await_group(l, group_of[group[0]])
        for w in fresh:
            transformed.add((l, w))
            spectrum(l, w)

    @scoped
    def convolve(l, group):
        for c in group:
            mix_bins(l, c)
        for c in group:
            invert(l, c)

    def await_swap(l, group):
        with jax.named_scope("swapwait"):
            whole(peer.at[l, span_rows(group)], swap_recv.at[l, group_of[group[0]]]).wait()

    def mix(l, group):
        rows = span_rows(group)
        need("cgain", "cshift")
        values = jnp.concatenate([conv[l, rows, :], peer[l, rows, :]], axis=-1).astype(jnp.float32)
        center = jnp.mean(values, axis=-1, keepdims=True)
        values = values - center
        spread = jnp.mean(values * values, axis=-1, keepdims=True)
        normed = values * lax.rsqrt(spread + 1e-05) * cgain_v[l : l + 1, :] + cshift_v[l : l + 1, :]
        return (normed * jax.nn.sigmoid(normed)).astype(jnp.bfloat16)

    @scoped
    def finish(l, group):
        rows = span_rows(group)
        last = l == layers - 1
        await_swap(l, group)
        need("cgain", "cshift", ("out", l))
        if not last:
            need(("gate", l + 1))
        mixed = mix(l, group)
        out = wo_last if last else wo_v.at[l]
        step = width // 4
        squares = 0.0
        for n in range(0, width, step):
            update = jnp.dot(mixed, out[:, n : n + step], preferred_element_type=jnp.float32)
            new = (x_v[rows, n : n + step].astype(jnp.float32) + update).astype(jnp.bfloat16)
            x_v[rows, n : n + step] = new
            if not last:
                x = new.astype(jnp.float32)
                squares = squares + jnp.sum(x * x, axis=-1, keepdims=True)
                gained[rows, n : n + step] = (x * gain_v[l + 1 : l + 2, n : n + step]).astype(jnp.bfloat16)
        if not last:
            gate(l + 1, group, squares)
            for c in group:
                send(l + 1, c)

    for c in range(plan.outs):
        gate(0, [c])
        if c == 0:
            with jax.named_scope("barrier"):
                pl.semaphore_wait(barrier, 1 + jnp.minimum(plan.n_sp - 1 - sp, len(hops)))
        send(0, c)
    for l in range(layers):
        transform_taps(l)
    need("bias")
    for l in range(layers):
        spectra_for(l, plan.groups[0], True)
        finished = 0
        for g, group in enumerate(plan.groups):
            spectra_for(l, group, False)
            convolve(l, group)
            if g:
                finish(l, plan.groups[finished])
                finished += 1
        for group in plan.groups[finished:-1] if l == layers - 1 else plan.groups[finished:]:
            finish(l, group)

    await_swap(layers - 1, plan.groups[-1])
    mixed_v[...] = mix(layers - 1, plan.groups[-1])
    whole(conv, swap_send.at[0]).wait()
    for h, hop in enumerate(hops):
        count = sum(piece[4] for piece in plan.pieces if piece[1] == hop)

        @pl.when(sp + hop < plan.n_sp)
        def _():
            whole(gated.at[:, pl.ds(0, count)], send_sem.at[h]).wait()


def last_out(done, x_v, mixed, wo, result, tail, sem):
    rows, width = tail.shape
    copies = [pltpu.make_async_copy(x_v.at[a:b], result.at[a:b], sem.at[0]) for a, b in done]
    for copy in copies:
        copy.start()
    step = width // 4
    for n in range(0, width, step):
        update = jnp.dot(mixed[...], wo[:, n : n + step], preferred_element_type=jnp.float32)
        tail[:, n : n + step] = (x_v[:rows, n : n + step].astype(jnp.float32) + update).astype(jnp.bfloat16)
        copy = pltpu.make_async_copy(tail.at[:, n : n + step], result.at[:rows, n : n + step], sem.at[0])
        copy.start()
        copies.append(copy)
    for copy in copies:
        copy.wait()


def per_device(stream, norm_gain, value_weight, gate_weight, conv_taps, conv_bias, channel_gain, channel_shift, out_weight):
    tokens, width = stream.shape
    layers, reach, half = conv_taps.shape
    plan = Plan(tokens, width, reach, lax.axis_size("sp"))
    mats = dft_matrices(BLOCK)
    n_hops = len({piece[1] for piece in plan.pieces})
    bf16, f32, dma = jnp.bfloat16, jnp.float32, pltpu.SemaphoreType.DMA
    windows = plan.parts + plan.outs - 1
    last_rows = sum(b - a for a, b in (plan.chunks[c] for c in plan.groups[-1]))
    x, mixed, wo_last = pl.pallas_call(
        functools.partial(kernel, plan, layers),
        out_shape=[
            pltpu.VMEM(stream.shape, stream.dtype),
            pltpu.VMEM((last_rows, 2 * half), bf16),
            pltpu.VMEM(out_weight.shape[1:], bf16),
        ],
        in_specs=[pl.BlockSpec(memory_space=pltpu.HBM)] * 10,
        out_specs=[pl.BlockSpec(memory_space=pltpu.VMEM)] * 3,
        scratch_shapes=[
            pltpu.VMEM(norm_gain.shape, f32),
            pltpu.VMEM((layers, width, 2 * half), bf16),
            pltpu.VMEM(conv_taps.shape, bf16),
            pltpu.VMEM(conv_bias.shape, f32),
            pltpu.VMEM(channel_gain.shape, f32),
            pltpu.VMEM(channel_shift.shape, f32),
            pltpu.VMEM((layers - 1, *out_weight.shape[1:]), bf16),
            pltpu.VMEM(mats.shape, bf16),
            pltpu.VMEM((layers, plan.rows, half), bf16),
            pltpu.VMEM((tokens, width), bf16),
            pltpu.VMEM((layers, windows, 2 * BLOCK, half), f32),
            pltpu.VMEM((layers, plan.parts, 2 * BLOCK, half), f32),
            pltpu.VMEM((plan.outs, 2 * BLOCK, half), bf16),
            pltpu.VMEM((layers, tokens, half), bf16),
            pltpu.VMEM((layers, tokens, half), bf16),
            dma((8 + 2 * layers,)),
            dma((n_hops,)),
            dma((layers, n_hops, len(plan.groups))),
            dma((1,)),
            dma((layers, len(plan.groups))),
        ],
        compiler_params=pltpu.CompilerParams(
            collective_id=0, has_side_effects=True, vmem_limit_bytes=61400 * 1024
        ),
    )(stream, norm_gain, value_weight, gate_weight, conv_taps, conv_bias, channel_gain, channel_shift, out_weight, mats)
    done = [(plan.chunks[c][0] - plan.own, plan.chunks[c][1] - plan.own) for g in plan.groups[:-1] for c in g]
    return pl.pallas_call(
        functools.partial(last_out, done),
        out_shape=jax.ShapeDtypeStruct(stream.shape, stream.dtype),
        in_specs=[pl.BlockSpec(memory_space=pltpu.VMEM)] * 3,
        out_specs=pl.BlockSpec(memory_space=pltpu.HBM),
        scratch_shapes=[pltpu.VMEM((last_rows, width), bf16), dma((1,))],
        compiler_params=pltpu.CompilerParams(vmem_limit_bytes=16000 * 1024),
    )(x, mixed, wo_last)


def solution(mesh):
    return jax.shard_map(
        per_device,
        mesh=mesh,
        in_specs=(
            P("sp", None),
            P(),
            P(None, None, "tp"),
            P(None, None, "tp"),
            P(None, None, "tp"),
            P(None, "tp"),
            P(),
            P(),
            P(),
        ),
        out_specs=P("sp", None),
        check_vma=False,
    )
```

```python
import functools

import jax
import jax.numpy as jnp
import numpy as np
from jax import lax
from jax.experimental import pallas as pl
from jax.experimental.pallas import tpu as pltpu
from jax.sharding import PartitionSpec as P

BLOCK = 128
STEPS = 4
LANES = 128
MESH = pl.DeviceIdType.MESH


def dft_matrices(block):
    span = 2 * block
    angle = 2 * np.pi / span * np.outer(np.arange(block) + 0.5, np.arange(span))
    forward = np.concatenate([np.cos(angle), -np.sin(angle)], axis=0)
    of_taps = forward[:, block - 1 :: -1]
    inverse = forward[:, block:].T / block
    of_taps = np.concatenate([of_taps, np.zeros_like(of_taps)], axis=1)
    return jnp.asarray(np.concatenate([forward, inverse, of_taps]), jnp.bfloat16)


class Plan:
    def __init__(self, tokens, width, reach, n_sp):
        self.tokens, self.n_sp = tokens, n_sp
        self.parts = reach // BLOCK
        self.outs = -(-tokens // BLOCK)
        self.rows = (self.parts + self.outs) * BLOCK
        self.own = self.rows - tokens
        low = self.own - reach
        self.chunks = []
        for p in reversed(range(self.outs)):
            start = (self.parts + p) * BLOCK
            self.chunks.append((max(start, self.own), start + BLOCK))
        self.groups = [[c] for c in range(self.outs - 2)] + [list(range(max(self.outs - 2, 0), self.outs))]
        self.pieces = []
        for c, (a, b) in enumerate(self.chunks):
            for hop in range(1, min(-(-reach // tokens), n_sp - 1) + 1):
                first, end = max(a, low + hop * tokens) - hop * tokens, b - hop * tokens
                while first < end:
                    cut = max(first, (end - 1) // BLOCK * BLOCK if end <= self.outs * BLOCK else first)
                    when = c if hop == 1 else max(self.outs - 3, 0)
                    self.pieces.append((when, hop, cut + hop * tokens, cut, end - cut))
                    end = cut
        self.pieces.sort(key=lambda piece: piece[:2])
        self.needs = []
        for _, _, _, target, count in self.pieces:
            for g, group in enumerate(self.groups):
                if target + count > (self.outs - 1 - group[-1]) * BLOCK:
                    self.needs.append(g)
                    break


def scoped(fn):
    def named(*args):
        label = "_".join(str(a) for a in args if isinstance(a, (int, list)))
        with jax.named_scope(f"{fn.__name__}#{label}"):
            return fn(*args)

    return named


def kernel(
    plan, layers, stream, gain, wv, wg, taps, bias, cgain, cshift, wo, mats, x_v, mixed_v, wo_last,
    gain_v, w_v, taps_v, bias_v, cgain_v, cshift_v, wo_v, mats_v,
    gated, gained, spectra, kernels, sums, freq, conv, peer, shift, load_sem, send_sem, recv_sem, swap_send, swap_recv, fence_sem,
):
    sp, tp = lax.axis_index("sp"), lax.axis_index("tp")
    half = wv.shape[2]
    width = x_v.shape[1]
    mine = pl.ds(pl.multiple_of(tp * half, half), half)
    other = pl.ds(pl.multiple_of((1 - tp) * half, half), half)
    first, second = pl.ds(0, half), pl.ds(half, half)
    loads = {}
    waited = set()

    def load(key, whole, *parts):
        sem = load_sem.at[len(loads)]
        loads[key] = pltpu.make_async_copy(whole, whole, sem)
        for source, target in parts:
            pltpu.make_async_copy(source, target, sem).start()

    def need(*keys):
        for key in keys:
            if key not in waited:
                waited.add(key)
                loads[key].wait()

    def own_rows(c):
        a, b = plan.chunks[c]
        return pl.ds(a - plan.own, b - a)

    def load_rows(key, a, b):
        rows = pl.ds(a, b - a)
        load(key, x_v.at[rows], (stream.at[rows], x_v.at[rows]))

    def load_gate(l, steps=1):
        for k in range(steps):
            depth = pl.ds(k * (width // steps), width // steps)
            parts = (wv.at[l, depth], w_v.at[l, depth, first]), (wg.at[l, depth], w_v.at[l, depth, second])
            load(("gate", l, k), w_v.at[l, depth], *parts)

    def load_halves(key, source, target):
        load(key, target, (source(mine), target.at[first]), (source(other), target.at[second]))

    head = plan.chunks[0][0] - plan.own
    load("gain", gain_v, (gain, gain_v))
    load_rows("x0", head, x_v.shape[0])
    load_gate(0, STEPS)
    load_rows("x", 0, head)
    load("taps", taps_v, (taps, taps_v))
    load("mats", mats_v, (mats, mats_v))
    load("bias", bias_v, (bias, bias_v))
    load("cgain", cgain_v, (cgain.at[:, mine], cgain_v.at[:, first]), (cgain.at[:, other], cgain_v.at[:, second]))
    load("cshift", cshift_v, (cshift.at[:, mine], cshift_v.at[:, first]), (cshift.at[:, other], cshift_v.at[:, second]))
    for l in range(layers):
        if l:
            load_gate(l)
        load_halves(("out", l), lambda channels: wo.at[l, channels], wo_last if l == layers - 1 else wo_v.at[l])
    fwd_v, inv_v = mats_v.at[: 2 * BLOCK], mats_v.at[2 * BLOCK : 3 * BLOCK]
    oft_v = mats_v.at[3 * BLOCK :, :BLOCK]

    for l in range(layers):
        gated[l, : plan.own] = jnp.zeros((plan.own, half), jnp.bfloat16)

    hops = sorted({piece[1] for piece in plan.pieces})
    barrier = pltpu.get_barrier_semaphore()
    pl.semaphore_signal(barrier, inc=1, device_id={"tp": 1 - tp}, device_id_type=MESH)
    for hop in hops:
        @pl.when(sp >= hop)
        def _():
            pl.semaphore_signal(barrier, inc=1, device_id={"sp": sp - hop}, device_id_type=MESH)

    def piece_copy(l, i):
        _, hop, source, target, count = plan.pieces[i]
        return pltpu.make_async_remote_copy(
            src_ref=gated.at[l, pl.ds(source, count)],
            dst_ref=gated.at[l, pl.ds(target, count)],
            send_sem=send_sem.at[hops.index(hop)],
            recv_sem=recv_sem.at[l, hops.index(hop), plan.needs[i]],
            device_id={"sp": sp + hop},
            device_id_type=MESH,
        )

    group_of = {c: g for g, group in enumerate(plan.groups) for c in group}

    def swap_copy(l, c):
        return pltpu.make_async_remote_copy(
            src_ref=conv.at[l, own_rows(c)],
            dst_ref=peer.at[l, own_rows(c)],
            send_sem=swap_send.at[0],
            recv_sem=swap_recv.at[l, group_of[c]],
            device_id={"tp": 1 - tp},
            device_id_type=MESH,
        )

    def span(group):
        return plan.chunks[group[-1]][0], plan.chunks[group[0]][1]

    def span_rows(group):
        a, b = span(group)
        return pl.ds(a - plan.own, b - a)

    @scoped
    def gate(l, group, squares=None):
        rows = span_rows(group)
        if squares is None:
            need("gain", "x" if group[0] else "x0")
            squares = 0.0
            step = width // 4
            for k in range(0, width, step):
                x = x_v[rows, k : k + step].astype(jnp.float32)
                squares = squares + jnp.sum(x * x, axis=-1, keepdims=True)
                gained[rows, k : k + step] = (x * gain_v[l : l + 1, k : k + step]).astype(jnp.bfloat16)
        if l == 0 and ("gate", 0, STEPS - 1) not in waited:
            both = 0.0
            for k in range(STEPS):
                depth = slice(k * (width // STEPS), (k + 1) * (width // STEPS))
                need(("gate", 0, k))
                both = both + jnp.dot(gained[rows, depth], w_v[l, depth], preferred_element_type=jnp.float32)
        else:
            both = jnp.dot(gained[rows, :], w_v[l], preferred_element_type=jnp.float32)
        both = both * lax.rsqrt(squares / width + 1e-06)
        a, b = span(group)
        gated[l, a:b, :] = (both[:, :half] * jax.nn.sigmoid(both[:, half:])).astype(jnp.bfloat16)

    @scoped
    def send(l, c):
        for i, piece in enumerate(plan.pieces):
            if piece[0] == c:
                @pl.when(sp + piece[1] < plan.n_sp)
                def _():
                    piece_copy(l, i).start()

    @scoped
    def transform_taps(l):
        need("taps", "mats")
        for j in range(plan.parts):
            first = (plan.parts - 1 - j) * BLOCK
            kernels[l, j] = jnp.dot(
                oft_v[...], taps_v[l, first : first + BLOCK, :], preferred_element_type=jnp.float32
            )

    def whole(ref, sem):
        return pltpu.make_async_copy(ref, ref, sem)

    def await_group(l, g):
        for h, hop in enumerate(hops):
            spans = [(piece[3], piece[3] + piece[4]) for i, piece in enumerate(plan.pieces) if plan.needs[i] == g and piece[1] == hop]
            if spans:
                low, high = min(a for a, _ in spans), max(b for _, b in spans)
                assert high - low == sum(b - a for a, b in spans)
                with jax.named_scope(f"recv{hop}_{g}"):
                    @pl.when(sp >= hop)
                    def _():
                        whole(gated.at[l, pl.ds(low, high - low)], recv_sem.at[l, h, g]).wait()

    @scoped
    def spectrum(l, w):
        first, last = w * BLOCK, (w + 2) * BLOCK
        spectra[l, w] = jnp.dot(fwd_v[...], gated[l, first:last, :], preferred_element_type=jnp.float32)

    summed = {}

    def add_bins(l, c, windows, final=False):
        p = plan.outs - 1 - c
        begun = (l, c) in summed
        summed[l, c] = True
        tile = 16
        for k in range(0, BLOCK, tile):
            low, high = slice(k, k + tile), slice(BLOCK + k, BLOCK + k + tile)
            real, imag = (sums[c, low, :], sums[c, high, :]) if begun else (None, None)
            for w in windows:
                j = plan.parts - 1 + p - w
                xr, xi = spectra[l, w, low, :], spectra[l, w, high, :]
                hr, hi = kernels[l, j, low, :], kernels[l, j, high, :]
                r, i = xr * hr - xi * hi, xr * hi + xi * hr
                real, imag = (r, i) if real is None else (real + r, imag + i)
            if final:
                freq[c, low, :] = real.astype(jnp.bfloat16)
                freq[c, high, :] = imag.astype(jnp.bfloat16)
            else:
                sums[c, low, :], sums[c, high, :] = real, imag

    unused = {(l, c): [w for w in reversed(range(plan.outs - 1 - c, plan.outs - 1 - c + plan.parts))] for l in range(layers) for c in range(plan.outs)}

    def add_ready(l, c, final=False):
        ready = [w for w in unused[l, c] if (l, w) in transformed]
        unused[l, c] = [w for w in unused[l, c] if w not in ready]
        assert not (final and unused[l, c])
        if ready or final:
            add_bins(l, c, ready, final)

    def add_later(l, groups):
        for group in groups:
            for c in group:
                add_ready(l, c)

    def fence():
        pl.semaphore_signal(fence_sem, 1)
        pl.semaphore_wait(fence_sem, 1)

    def invert(l, c):
        a, b = plan.chunks[c]
        result = jnp.dot(inv_v[BLOCK - (b - a) :, :], freq[c], preferred_element_type=jnp.float32)
        conv[l, own_rows(c), :] = (result + bias_v[l : l + 1, :]).astype(jnp.bfloat16)
        swap_copy(l, c).start()

    transformed = set()

    def spectra_for(l, group, own):
        p = plan.outs - 1 - group[-1]
        q = plan.outs - 1 - group[0]
        fresh = [w for w in range(p, q + plan.parts) if (l, w) not in transformed]
        fresh = [w for w in reversed(fresh) if not own or w * BLOCK >= plan.own]
        if not own:
            await_group(l, group_of[group[0]])
        for w in fresh:
            transformed.add((l, w))
            spectrum(l, w)

    @scoped
    def convolve(l, group):
        for c in group:
            add_ready(l, c, final=True)
        for c in group:
            invert(l, c)

    def await_swap(l, group):
        with jax.named_scope("swapwait"):
            whole(peer.at[l, span_rows(group)], swap_recv.at[l, group_of[group[0]]]).wait()

    def own_mean(l, group):
        rows = span_rows(group)
        mean = jnp.mean(conv[l, rows, :].astype(jnp.float32), axis=-1, keepdims=True)
        shift[l, rows, :] = jnp.broadcast_to(mean, (mean.shape[0], LANES))

    def mix(l, group):
        rows = span_rows(group)
        need("cgain", "cshift")
        values = jnp.concatenate([conv[l, rows, :], peer[l, rows, :]], axis=-1).astype(jnp.float32)
        channels = values.shape[1]
        values = values - jnp.concatenate([shift[l, rows, :]] * (channels // LANES), axis=-1)
        center = jnp.sum(values, axis=-1, keepdims=True) / channels
        spread = jnp.sum(values * values, axis=-1, keepdims=True) / channels - center * center
        scale = lax.rsqrt(jnp.maximum(spread, 0.0) + 1e-05)
        normed = (values - center) * scale * cgain_v[l : l + 1, :] + cshift_v[l : l + 1, :]
        return (normed * jax.nn.sigmoid(normed)).astype(jnp.bfloat16)

    @scoped
    def finish(l, group, after=None):
        rows = span_rows(group)
        last = l == layers - 1
        await_swap(l, group)
        need("cgain", "cshift", ("out", l))
        if not last:
            need(("gate", l + 1, 0))
        if after:
            own_mean(l, after)
        mixed = mix(l, group)
        out = wo_last if last else wo_v.at[l]
        step = width // 4
        squares = 0.0
        for n in range(0, width, step):
            update = jnp.dot(mixed, out[:, n : n + step], preferred_element_type=jnp.float32)
            new = (x_v[rows, n : n + step].astype(jnp.float32) + update).astype(jnp.bfloat16)
            x_v[rows, n : n + step] = new
            if not last:
                x = new.astype(jnp.float32)
                squares = squares + jnp.sum(x * x, axis=-1, keepdims=True)
                gained[rows, n : n + step] = (x * gain_v[l + 1 : l + 2, n : n + step]).astype(jnp.bfloat16)
        if not last:
            gate(l + 1, group, squares)
        add_later(l, plan.groups)
        if not last:
            for c in group:
                send(l + 1, c)

    for c in range(plan.outs):
        gate(0, [c])
        if c == 0:
            with jax.named_scope("barrier"):
                pl.semaphore_wait(barrier, 1 + jnp.minimum(plan.n_sp - 1 - sp, len(hops)))
        send(0, c)
    for l in range(layers):
        transform_taps(l)
    need("bias")
    for l in range(layers):
        last = l == layers - 1
        spectra_for(l, plan.groups[0], True)
        add_later(l, plan.groups)
        for g, group in enumerate(plan.groups):
            spectra_for(l, group, False)
            if g:
                own_mean(l, plan.groups[g - 1])
            convolve(l, group)
            if g == 0:
                fence()
                add_later(l, plan.groups[1:])
            else:
                finish(l, plan.groups[g - 1], group if group is plan.groups[-1] else None)
        if not last:
            finish(l, plan.groups[-1])

    await_swap(layers - 1, plan.groups[-1])
    mixed_v[...] = mix(layers - 1, plan.groups[-1])
    whole(conv, swap_send.at[0]).wait()
    for h, hop in enumerate(hops):
        count = sum(piece[4] for piece in plan.pieces if piece[1] == hop)

        @pl.when(sp + hop < plan.n_sp)
        def _():
            whole(gated.at[:, pl.ds(0, count)], send_sem.at[h]).wait()


def last_out(done, x_v, mixed, wo, result, tail, sem):
    rows, width = tail.shape
    copies = [pltpu.make_async_copy(x_v.at[a:b], result.at[a:b], sem.at[0]) for a, b in done]
    for copy in copies:
        copy.start()
    step = width // 4
    for n in range(0, width, step):
        update = jnp.dot(mixed[...], wo[:, n : n + step], preferred_element_type=jnp.float32)
        tail[:, n : n + step] = (x_v[:rows, n : n + step].astype(jnp.float32) + update).astype(jnp.bfloat16)
        copy = pltpu.make_async_copy(tail.at[:, n : n + step], result.at[:rows, n : n + step], sem.at[0])
        copy.start()
        copies.append(copy)
    for copy in copies:
        copy.wait()


def per_device(stream, norm_gain, value_weight, gate_weight, conv_taps, conv_bias, channel_gain, channel_shift, out_weight):
    tokens, width = stream.shape
    layers, reach, half = conv_taps.shape
    plan = Plan(tokens, width, reach, lax.axis_size("sp"))
    mats = dft_matrices(BLOCK)
    n_hops = len({piece[1] for piece in plan.pieces})
    bf16, f32, dma = jnp.bfloat16, jnp.float32, pltpu.SemaphoreType.DMA
    windows = plan.parts + plan.outs - 1
    last_rows = sum(b - a for a, b in (plan.chunks[c] for c in plan.groups[-1]))
    x, mixed, wo_last = pl.pallas_call(
        functools.partial(kernel, plan, layers),
        out_shape=[
            pltpu.VMEM(stream.shape, stream.dtype),
            pltpu.VMEM((last_rows, 2 * half), bf16),
            pltpu.VMEM(out_weight.shape[1:], bf16),
        ],
        in_specs=[pl.BlockSpec(memory_space=pltpu.HBM)] * 10,
        out_specs=[pl.BlockSpec(memory_space=pltpu.VMEM)] * 3,
        scratch_shapes=[
            pltpu.VMEM(norm_gain.shape, f32),
            pltpu.VMEM((layers, width, 2 * half), bf16),
            pltpu.VMEM(conv_taps.shape, bf16),
            pltpu.VMEM(conv_bias.shape, f32),
            pltpu.VMEM(channel_gain.shape, f32),
            pltpu.VMEM(channel_shift.shape, f32),
            pltpu.VMEM((layers - 1, *out_weight.shape[1:]), bf16),
            pltpu.VMEM(mats.shape, bf16),
            pltpu.VMEM((layers, plan.rows, half), bf16),
            pltpu.VMEM((tokens, width), bf16),
            pltpu.VMEM((layers, windows, 2 * BLOCK, half), f32),
            pltpu.VMEM((layers, plan.parts, 2 * BLOCK, half), f32),
            pltpu.VMEM((plan.outs, 2 * BLOCK, half), f32),
            pltpu.VMEM((plan.outs, 2 * BLOCK, half), bf16),
            pltpu.VMEM((layers, tokens, half), bf16),
            pltpu.VMEM((layers, tokens, half), bf16),
            pltpu.VMEM((layers, tokens, LANES), f32),
            dma((7 + STEPS + 2 * layers,)),
            dma((n_hops,)),
            dma((layers, n_hops, len(plan.groups))),
            dma((1,)),
            dma((layers, len(plan.groups))),
            pltpu.SemaphoreType.REGULAR,
        ],
        compiler_params=pltpu.CompilerParams(
            collective_id=0, has_side_effects=True, vmem_limit_bytes=61400 * 1024
        ),
    )(stream, norm_gain, value_weight, gate_weight, conv_taps, conv_bias, channel_gain, channel_shift, out_weight, mats)
    done = [(plan.chunks[c][0] - plan.own, plan.chunks[c][1] - plan.own) for g in plan.groups[:-1] for c in g]
    return pl.pallas_call(
        functools.partial(last_out, done),
        out_shape=jax.ShapeDtypeStruct(stream.shape, stream.dtype),
        in_specs=[pl.BlockSpec(memory_space=pltpu.VMEM)] * 3,
        out_specs=pl.BlockSpec(memory_space=pltpu.HBM),
        scratch_shapes=[pltpu.VMEM((last_rows, width), bf16), dma((1,))],
        compiler_params=pltpu.CompilerParams(vmem_limit_bytes=16000 * 1024),
    )(x, mixed, wo_last)


def solution(mesh):
    return jax.shard_map(
        per_device,
        mesh=mesh,
        in_specs=(
            P("sp", None),
            P(),
            P(None, None, "tp"),
            P(None, None, "tp"),
            P(None, None, "tp"),
            P(None, "tp"),
            P(),
            P(),
            P(),
        ),
        out_specs=P("sp", None),
        check_vma=False,
    )
```

```python
import functools

import jax
import jax.numpy as jnp
import numpy as np
from jax import lax
from jax.experimental import pallas as pl
from jax.experimental.pallas import tpu as pltpu
from jax.sharding import PartitionSpec as P

BLOCK = 128
STEPS = 4
ORDER = [("conv", [0]), ("conv", [1]), ("out", [0]), ("conv", [2]), ("out", [1]), ("conv", [3]), ("out", [2]), ("out", [3])]
ORDER_LAST = [("conv", [0]), ("conv", [1]), ("out", [0]), ("conv", [2]), ("conv", [3]), ("out", [1]), ("out", [2])]
LANES = 128
MESH = pl.DeviceIdType.MESH


def dft_matrices(block):
    span = 2 * block
    angle = 2 * np.pi / span * np.outer(np.arange(block) + 0.5, np.arange(span))
    forward = np.concatenate([np.cos(angle), -np.sin(angle)], axis=0)
    of_taps = forward[:, block - 1 :: -1]
    inverse = forward[:, block:].T / block
    of_taps = np.concatenate([of_taps, np.zeros_like(of_taps)], axis=1)
    return jnp.asarray(np.concatenate([forward, inverse, of_taps]), jnp.bfloat16)


class Plan:
    def __init__(self, tokens, width, reach, n_sp):
        self.tokens, self.n_sp = tokens, n_sp
        self.parts = reach // BLOCK
        self.outs = -(-tokens // BLOCK)
        self.rows = (self.parts + self.outs) * BLOCK
        self.own = self.parts * BLOCK
        low = self.own - reach
        self.chunks = []
        for p in reversed(range(self.outs)):
            start = (self.parts + p) * BLOCK
            self.chunks.append((start, min(start + BLOCK, self.own + tokens)))
        self.groups = [[c] for c in range(self.outs)]
        self.tail = list(range(max(self.outs - 1, 0), self.outs))
        self.pieces = []
        for c, (a, b) in enumerate(self.chunks):
            for hop in range(1, min(-(-reach // tokens), n_sp - 1) + 1):
                first, end = max(a, low + hop * tokens) - hop * tokens, b - hop * tokens
                while first < end:
                    cut = max(first, (end - 1) // BLOCK * BLOCK if hop == 1 else first)
                    when = c if hop == 1 else max(self.outs - 3, 0)
                    self.pieces.append((when, hop, cut + hop * tokens, cut, end - cut))
                    end = cut
        self.pieces.sort(key=lambda piece: piece[:2])
        self.needs = []
        for _, _, _, target, count in self.pieces:
            for g, group in enumerate(self.groups):
                if target + count > (self.outs - 1 - group[-1]) * BLOCK:
                    self.needs.append(g)
                    break
        self.slots = sorted({(piece[1], need) for piece, need in zip(self.pieces, self.needs)})


def scoped(fn):
    def named(*args):
        label = "_".join(str(a) for a in args if isinstance(a, (int, list)))
        with jax.named_scope(f"{fn.__name__}#{label}"):
            return fn(*args)

    return named


def kernel(
    plan, layers, stream, gain, wv, wg, taps, bias, cgain, cshift, wo, mats, x_v, mixed_v, wo_last,
    gain_v, w_v, taps_v, bias_v, cgain_v, cshift_v, wo_v, mats_v,
    gated, gained, spectra, kernels, sums, freq, conv, peer, shift, load_sem, send_sem, recv_sem, swap_send, swap_recv, fence_sem,
):
    sp, tp = lax.axis_index("sp"), lax.axis_index("tp")
    half = wv.shape[2]
    width = x_v.shape[1]
    mine = pl.ds(pl.multiple_of(tp * half, half), half)
    other = pl.ds(pl.multiple_of((1 - tp) * half, half), half)
    first, second = pl.ds(0, half), pl.ds(half, half)
    loads = {}
    waited = set()

    def load(key, whole, *parts):
        sem = load_sem.at[len(loads)]
        loads[key] = pltpu.make_async_copy(whole, whole, sem)
        for source, target in parts:
            pltpu.make_async_copy(source, target, sem).start()

    def need(*keys):
        for key in keys:
            if key not in waited:
                waited.add(key)
                loads[key].wait()

    def own_rows(c):
        a, b = plan.chunks[c]
        return pl.ds(a - plan.own, b - a)

    def load_rows(key, a, b):
        rows = pl.ds(a, b - a)
        load(key, x_v.at[rows], (stream.at[rows], x_v.at[rows]))

    def load_gate(l, steps=1):
        for k in range(steps):
            depth = pl.ds(k * (width // steps), width // steps)
            parts = (wv.at[l, depth], w_v.at[l, depth, first]), (wg.at[l, depth], w_v.at[l, depth, second])
            load(("gate", l, k), w_v.at[l, depth], *parts)

    def load_halves(key, source, target):
        load(key, target, (source(mine), target.at[first]), (source(other), target.at[second]))

    head = plan.chunks[0][0] - plan.own
    load("gain", gain_v, (gain, gain_v))
    load_rows("x0", head, x_v.shape[0])
    load_gate(0, STEPS)
    load_rows("x", 0, head)
    load("taps", taps_v, (taps, taps_v))
    load("mats", mats_v, (mats, mats_v))
    load("bias", bias_v, (bias, bias_v))
    load("cgain", cgain_v, (cgain.at[:, mine], cgain_v.at[:, first]), (cgain.at[:, other], cgain_v.at[:, second]))
    load("cshift", cshift_v, (cshift.at[:, mine], cshift_v.at[:, first]), (cshift.at[:, other], cshift_v.at[:, second]))
    for l in range(layers):
        if l:
            load_gate(l)
        load_halves(("out", l), lambda channels: wo.at[l, channels], wo_last if l == layers - 1 else wo_v.at[l])
    fwd_v, inv_v = mats_v.at[: 2 * BLOCK], mats_v.at[2 * BLOCK : 3 * BLOCK]
    oft_v = mats_v.at[3 * BLOCK :, :BLOCK]

    for l in range(layers):
        end = plan.own + x_v.shape[0]
        gated[l, : plan.own] = jnp.zeros((plan.own, half), jnp.bfloat16)
        gated[l, end:] = jnp.zeros((plan.rows - end, half), jnp.bfloat16)

    hops = sorted({piece[1] for piece in plan.pieces})
    barrier = pltpu.get_barrier_semaphore()
    pl.semaphore_signal(barrier, inc=1, device_id={"tp": 1 - tp}, device_id_type=MESH)
    for hop in hops:
        @pl.when(sp >= hop)
        def _():
            pl.semaphore_signal(barrier, inc=1, device_id={"sp": sp - hop}, device_id_type=MESH)

    def piece_copy(l, i):
        _, hop, source, target, count = plan.pieces[i]
        return pltpu.make_async_remote_copy(
            src_ref=gated.at[l, pl.ds(source, count)],
            dst_ref=gated.at[l, pl.ds(target, count)],
            send_sem=send_sem.at[hops.index(hop)],
            recv_sem=recv_sem.at[l, plan.slots.index((hop, plan.needs[i]))],
            device_id={"sp": sp + hop},
            device_id_type=MESH,
        )

    group_of = {c: g for g, group in enumerate(plan.groups) for c in group}

    def swap_copy(l, c):
        return pltpu.make_async_remote_copy(
            src_ref=conv.at[l, own_rows(c)],
            dst_ref=peer.at[l, own_rows(c)],
            send_sem=swap_send.at[0],
            recv_sem=swap_recv.at[l, group_of[c]],
            device_id={"tp": 1 - tp},
            device_id_type=MESH,
        )

    def span(group):
        return plan.chunks[group[-1]][0], plan.chunks[group[0]][1]

    def span_rows(group):
        a, b = span(group)
        return pl.ds(a - plan.own, b - a)

    @scoped
    def gate(l, group, squares=None):
        rows = span_rows(group)
        if squares is None:
            need("gain", "x" if group[0] else "x0")
            squares = 0.0
            step = width // 4
            for k in range(0, width, step):
                x = x_v[rows, k : k + step].astype(jnp.float32)
                squares = squares + jnp.sum(x * x, axis=-1, keepdims=True)
                gained[rows, k : k + step] = (x * gain_v[l : l + 1, k : k + step]).astype(jnp.bfloat16)
        if l == 0 and ("gate", 0, STEPS - 1) not in waited:
            both = 0.0
            for k in range(STEPS):
                depth = slice(k * (width // STEPS), (k + 1) * (width // STEPS))
                need(("gate", 0, k))
                both = both + jnp.dot(gained[rows, depth], w_v[l, depth], preferred_element_type=jnp.float32)
        else:
            both = jnp.dot(gained[rows, :], w_v[l], preferred_element_type=jnp.float32)
        both = both * lax.rsqrt(squares / width + 1e-06)
        a, b = span(group)
        gated[l, a:b, :] = (both[:, :half] * jax.nn.sigmoid(both[:, half:])).astype(jnp.bfloat16)

    @scoped
    def send(l, c):
        for i, piece in enumerate(plan.pieces):
            if piece[0] == c:
                @pl.when(sp + piece[1] < plan.n_sp)
                def _():
                    piece_copy(l, i).start()

    @scoped
    def transform_taps(l):
        need("taps", "mats")
        for j in range(plan.parts):
            first = (plan.parts - 1 - j) * BLOCK
            kernels[l, j] = jnp.dot(
                oft_v[...], taps_v[l, first : first + BLOCK, :], preferred_element_type=jnp.float32
            )

    def whole(ref, sem):
        return pltpu.make_async_copy(ref, ref, sem)

    def await_group(l, g):
        for h, hop in enumerate(hops):
            spans = [(piece[3], piece[3] + piece[4]) for i, piece in enumerate(plan.pieces) if plan.needs[i] == g and piece[1] == hop]
            if spans:
                low, high = min(a for a, _ in spans), max(b for _, b in spans)
                assert high - low == sum(b - a for a, b in spans)
                with jax.named_scope(f"recv{hop}_{g}"):
                    @pl.when(sp >= hop)
                    def _():
                        whole(gated.at[l, pl.ds(low, high - low)], recv_sem.at[l, plan.slots.index((hop, g))]).wait()

    @scoped
    def spectrum(l, w):
        first, last = w * BLOCK, (w + 2) * BLOCK
        spectra[l, w] = jnp.dot(fwd_v[...], gated[l, first:last, :], preferred_element_type=jnp.float32)

    summed = {}

    def add_bins(l, c, windows, final=False):
        p = plan.outs - 1 - c
        begun = (l, c) in summed
        summed[l, c] = True
        tile = 16
        for k in range(0, BLOCK, tile):
            low, high = slice(k, k + tile), slice(BLOCK + k, BLOCK + k + tile)
            real, imag = (sums[c, low, :], sums[c, high, :]) if begun else (None, None)
            for w in windows:
                j = plan.parts - 1 + p - w
                xr, xi = spectra[l, w, low, :], spectra[l, w, high, :]
                hr, hi = kernels[l, j, low, :], kernels[l, j, high, :]
                r, i = xr * hr - xi * hi, xr * hi + xi * hr
                real, imag = (r, i) if real is None else (real + r, imag + i)
            if final:
                freq[c, low, :] = real.astype(jnp.bfloat16)
                freq[c, high, :] = imag.astype(jnp.bfloat16)
            else:
                sums[c, low, :], sums[c, high, :] = real, imag

    unused = {(l, c): [w for w in reversed(range(plan.outs - 1 - c, plan.outs - 1 - c + plan.parts))] for l in range(layers) for c in range(plan.outs)}

    def add_ready(l, c, final=False):
        ready = [w for w in unused[l, c] if (l, w) in transformed]
        unused[l, c] = [w for w in unused[l, c] if w not in ready]
        assert not (final and unused[l, c])
        if ready or final:
            add_bins(l, c, ready, final)

    def add_later(l, groups):
        for group in groups:
            for c in group:
                add_ready(l, c)

    def fence():
        pl.semaphore_signal(fence_sem, 1)
        pl.semaphore_wait(fence_sem, 1)

    def invert(l, c):
        a, b = plan.chunks[c]
        result = jnp.dot(inv_v[: b - a, :], freq[c], preferred_element_type=jnp.float32)
        conv[l, own_rows(c), :] = (result + bias_v[l : l + 1, :]).astype(jnp.bfloat16)
        swap_copy(l, c).start()

    transformed = set()

    def spectra_for(l, group, own):
        p = plan.outs - 1 - group[-1]
        q = plan.outs - 1 - group[0]
        fresh = [w for w in range(p, q + plan.parts) if (l, w) not in transformed]
        fresh = [w for w in reversed(fresh) if not own or w * BLOCK >= plan.own]
        if not own:
            await_group(l, group_of[group[0]])
        for w in fresh:
            transformed.add((l, w))
            spectrum(l, w)

    @scoped
    def convolve(l, group):
        for c in group:
            add_ready(l, c, final=True)
        for c in group:
            invert(l, c)

    def await_swap(l, group):
        with jax.named_scope("swapwait"):
            whole(peer.at[l, span_rows(group)], swap_recv.at[l, group_of[group[0]]]).wait()

    def own_mean(l, group):
        rows = span_rows(group)
        mean = jnp.mean(conv[l, rows, :].astype(jnp.float32), axis=-1, keepdims=True)
        shift[l, rows, :] = jnp.broadcast_to(mean, (mean.shape[0], LANES))

    def mix(l, group):
        rows = span_rows(group)
        need("cgain", "cshift")
        values = jnp.concatenate([conv[l, rows, :], peer[l, rows, :]], axis=-1).astype(jnp.float32)
        channels = values.shape[1]
        values = values - jnp.concatenate([shift[l, rows, :]] * (channels // LANES), axis=-1)
        center = jnp.sum(values, axis=-1, keepdims=True) / channels
        spread = jnp.sum(values * values, axis=-1, keepdims=True) / channels - center * center
        scale = lax.rsqrt(jnp.maximum(spread, 0.0) + 1e-05)
        normed = (values - center) * scale * cgain_v[l : l + 1, :] + cshift_v[l : l + 1, :]
        return (normed * jax.nn.sigmoid(normed)).astype(jnp.bfloat16)

    swapped = set()

    @scoped
    def finish(l, group, unmeaned):
        rows = span_rows(group)
        last = l == layers - 1
        for g in sorted({group_of[c] for c in group}):
            if (l, g) not in swapped:
                swapped.add((l, g))
                await_swap(l, plan.groups[g])
        for part in unmeaned:
            if group_of[part[0]] in {group_of[c] for c in group}:
                own_mean(l, part)
        need("cgain", "cshift", ("out", l))
        if not last:
            need(("gate", l + 1, 0))
        for part in unmeaned:
            if group_of[part[0]] not in {group_of[c] for c in group}:
                own_mean(l, part)
        mixed = mix(l, group)
        out = wo_last if last else wo_v.at[l]
        step = width // 4
        squares = 0.0
        for n in range(0, width, step):
            update = jnp.dot(mixed, out[:, n : n + step], preferred_element_type=jnp.float32)
            new = (x_v[rows, n : n + step].astype(jnp.float32) + update).astype(jnp.bfloat16)
            x_v[rows, n : n + step] = new
            if not last:
                x = new.astype(jnp.float32)
                squares = squares + jnp.sum(x * x, axis=-1, keepdims=True)
                gained[rows, n : n + step] = (x * gain_v[l + 1 : l + 2, n : n + step]).astype(jnp.bfloat16)
        if not last:
            gate(l + 1, group, squares)
        add_later(l, plan.groups)
        if not last:
            for c in group:
                send(l + 1, c)

    for c in range(plan.outs):
        gate(0, [c])
        if c == 0:
            with jax.named_scope("barrier"):
                pl.semaphore_wait(barrier, 1 + jnp.minimum(plan.n_sp - 1 - sp, len(hops)))
        send(0, c)
    for l in range(layers):
        transform_taps(l)
    need("bias")
    for l in range(layers):
        spectra_for(l, plan.groups[0], True)
        add_later(l, plan.groups)
        unmeaned = []
        for step, which in ORDER_LAST if l == layers - 1 else ORDER:
            if step == "conv":
                group = plan.groups[which[0]]
                spectra_for(l, group, False)
                for part in unmeaned:
                    own_mean(l, part)
                convolve(l, group)
                unmeaned = [group]
                if which == [0]:
                    fence()
                    add_later(l, plan.groups[1:])
            else:
                finish(l, which, unmeaned)
                unmeaned = []

    for c in plan.tail:
        await_swap(layers - 1, [c])
        if [c] in unmeaned:
            own_mean(layers - 1, [c])
        mixed_v[own_rows(c)] = mix(layers - 1, [c])
    whole(conv, swap_send.at[0]).wait()
    for h, hop in enumerate(hops):
        count = sum(piece[4] for piece in plan.pieces if piece[1] == hop)

        @pl.when(sp + hop < plan.n_sp)
        def _():
            whole(gated.at[:, pl.ds(0, count)], send_sem.at[h]).wait()


def last_out(done, x_v, mixed, wo, result, tail, sem):
    rows, width = tail.shape
    copies = [pltpu.make_async_copy(x_v.at[a:b], result.at[a:b], sem.at[0]) for a, b in done]
    for copy in copies:
        copy.start()
    step = width // 4
    for n in range(0, width, step):
        update = jnp.dot(mixed[...], wo[:, n : n + step], preferred_element_type=jnp.float32)
        tail[:, n : n + step] = (x_v[:rows, n : n + step].astype(jnp.float32) + update).astype(jnp.bfloat16)
        copy = pltpu.make_async_copy(tail.at[:, n : n + step], result.at[:rows, n : n + step], sem.at[0])
        copy.start()
        copies.append(copy)
    for copy in copies:
        copy.wait()


def per_device(stream, norm_gain, value_weight, gate_weight, conv_taps, conv_bias, channel_gain, channel_shift, out_weight):
    tokens, width = stream.shape
    layers, reach, half = conv_taps.shape
    plan = Plan(tokens, width, reach, lax.axis_size("sp"))
    mats = dft_matrices(BLOCK)
    n_hops = len({piece[1] for piece in plan.pieces})
    bf16, f32, dma = jnp.bfloat16, jnp.float32, pltpu.SemaphoreType.DMA
    windows = plan.parts + plan.outs - 1
    last_rows = sum(b - a for a, b in (plan.chunks[c] for c in plan.tail))
    x, mixed, wo_last = pl.pallas_call(
        functools.partial(kernel, plan, layers),
        out_shape=[
            pltpu.VMEM(stream.shape, stream.dtype),
            pltpu.VMEM((last_rows, 2 * half), bf16),
            pltpu.VMEM(out_weight.shape[1:], bf16),
        ],
        in_specs=[pl.BlockSpec(memory_space=pltpu.HBM)] * 10,
        out_specs=[pl.BlockSpec(memory_space=pltpu.VMEM)] * 3,
        scratch_shapes=[
            pltpu.VMEM(norm_gain.shape, f32),
            pltpu.VMEM((layers, width, 2 * half), bf16),
            pltpu.VMEM(conv_taps.shape, bf16),
            pltpu.VMEM(conv_bias.shape, f32),
            pltpu.VMEM(channel_gain.shape, f32),
            pltpu.VMEM(channel_shift.shape, f32),
            pltpu.VMEM((layers - 1, *out_weight.shape[1:]), bf16),
            pltpu.VMEM(mats.shape, bf16),
            pltpu.VMEM((layers, plan.rows, half), bf16),
            pltpu.VMEM((tokens, width), bf16),
            pltpu.VMEM((layers, windows, 2 * BLOCK, half), f32),
            pltpu.VMEM((layers, plan.parts, 2 * BLOCK, half), f32),
            pltpu.VMEM((plan.outs, 2 * BLOCK, half), f32),
            pltpu.VMEM((plan.outs, 2 * BLOCK, half), bf16),
            pltpu.VMEM((layers, tokens, half), bf16),
            pltpu.VMEM((layers, tokens, half), bf16),
            pltpu.VMEM((layers, tokens, LANES), f32),
            dma((7 + STEPS + 2 * layers,)),
            dma((n_hops,)),
            dma((layers, len(plan.slots))),
            dma((1,)),
            dma((layers, len(plan.groups))),
            pltpu.SemaphoreType.REGULAR,
        ],
        compiler_params=pltpu.CompilerParams(
            collective_id=0, has_side_effects=True, vmem_limit_bytes=61300 * 1024
        ),
    )(stream, norm_gain, value_weight, gate_weight, conv_taps, conv_bias, channel_gain, channel_shift, out_weight, mats)
    done = [(plan.chunks[c][0] - plan.own, plan.chunks[c][1] - plan.own) for c in range(plan.outs) if c not in plan.tail]
    return pl.pallas_call(
        functools.partial(last_out, done),
        out_shape=jax.ShapeDtypeStruct(stream.shape, stream.dtype),
        in_specs=[pl.BlockSpec(memory_space=pltpu.VMEM)] * 3,
        out_specs=pl.BlockSpec(memory_space=pltpu.HBM),
        scratch_shapes=[pltpu.VMEM((last_rows, width), bf16), dma((1,))],
        compiler_params=pltpu.CompilerParams(vmem_limit_bytes=16000 * 1024),
    )(x, mixed, wo_last)


def solution(mesh):
    return jax.shard_map(
        per_device,
        mesh=mesh,
        in_specs=(
            P("sp", None),
            P(),
            P(None, None, "tp"),
            P(None, None, "tp"),
            P(None, None, "tp"),
            P(None, "tp"),
            P(),
            P(),
            P(),
        ),
        out_specs=P("sp", None),
        check_vma=False,
    )
```

```python
import functools

import jax
import jax.numpy as jnp
import numpy as np
from jax import lax
from jax.experimental import pallas as pl
from jax.experimental.pallas import tpu as pltpu
from jax.sharding import PartitionSpec as P

BLOCK = 128
STEPS = 4
ORDER = [("conv", [0]), ("conv", [1]), ("out", [0]), ("conv", [2]), ("out", [1]), ("conv", [3]), ("out", [2]), ("out", [3])]
ORDER_LAST = [("conv", [0]), ("conv", [1]), ("out", [0]), ("conv", [2]), ("conv", [3]), ("out", [1]), ("out", [2])]
LANES = 128
MESH = pl.DeviceIdType.MESH


def dft_matrices(block):
    span = 2 * block
    angle = 2 * np.pi / span * np.outer(np.arange(block) + 0.5, np.arange(span))
    forward = np.concatenate([np.cos(angle), -np.sin(angle)], axis=0)
    of_taps = forward[:, block - 1 :: -1]
    inverse = forward[:, block:].T / block
    of_taps = np.concatenate([of_taps, np.zeros_like(of_taps)], axis=1)
    return jnp.asarray(np.concatenate([forward, inverse, of_taps]), jnp.bfloat16)


class Plan:
    def __init__(self, tokens, width, reach, n_sp):
        self.tokens, self.n_sp = tokens, n_sp
        self.parts = reach // BLOCK
        self.outs = -(-tokens // BLOCK)
        self.rows = (self.parts + self.outs) * BLOCK
        self.own = self.parts * BLOCK
        low = self.own - reach
        self.chunks = []
        for p in reversed(range(self.outs)):
            start = (self.parts + p) * BLOCK
            self.chunks.append((start, min(start + BLOCK, self.own + tokens)))
        self.groups = [[c] for c in range(self.outs)]
        self.tail = list(range(max(self.outs - 1, 0), self.outs))
        self.pieces = []
        for c, (a, b) in enumerate(self.chunks):
            for hop in range(1, min(-(-reach // tokens), n_sp - 1) + 1):
                first, end = max(a, low + hop * tokens) - hop * tokens, b - hop * tokens
                while first < end:
                    cut = max(first, (end - 1) // BLOCK * BLOCK if hop == 1 else first)
                    when = c if hop == 1 else max(self.outs - 3, 0)
                    self.pieces.append((when, hop, cut + hop * tokens, cut, end - cut))
                    end = cut
        self.pieces.sort(key=lambda piece: piece[:2])
        self.needs = []
        for _, _, _, target, count in self.pieces:
            for g, group in enumerate(self.groups):
                if target + count > (self.outs - 1 - group[-1]) * BLOCK:
                    self.needs.append(g)
                    break
        self.slots = sorted({(piece[1], need) for piece, need in zip(self.pieces, self.needs)})


def scoped(fn):
    def named(*args):
        label = "_".join(str(a) for a in args if isinstance(a, (int, list)))
        with jax.named_scope(f"{fn.__name__}#{label}"):
            return fn(*args)

    return named


def kernel(
    plan, layers, stream, gain, wv, wg, taps, bias, cgain, cshift, wo, mats, x_v, mixed_v, wo_last,
    gain_v, w_v, taps_v, bias_v, cgain_v, cshift_v, wo_v, mats_v,
    gated, gained, spectra, kernels, sums, freq, conv, peer, shift, load_sem, send_sem, recv_sem, swap_send, swap_recv, fence_sem,
):
    sp, tp = lax.axis_index("sp"), lax.axis_index("tp")
    half = wv.shape[2]
    width = x_v.shape[1]
    mine = pl.ds(pl.multiple_of(tp * half, half), half)
    other = pl.ds(pl.multiple_of((1 - tp) * half, half), half)
    first, second = pl.ds(0, half), pl.ds(half, half)
    loads = {}
    free = list(range(load_sem.shape[0]))
    waited = set()

    def load(key, whole, *parts):
        sem = load_sem.at[free.pop(0)]
        loads[key] = pltpu.make_async_copy(whole, whole, sem)
        for source, target in parts:
            pltpu.make_async_copy(source, target, sem).start()

    def need(*keys):
        for key in keys:
            if key not in waited:
                waited.add(key)
                loads[key].wait()

    def own_rows(c):
        a, b = plan.chunks[c]
        return pl.ds(a - plan.own, b - a)

    def load_rows(key, a, b):
        rows = pl.ds(a, b - a)
        load(key, x_v.at[rows], (stream.at[rows], x_v.at[rows]))

    def load_gate(l, steps=1):
        for k in range(steps):
            depth = pl.ds(k * (width // steps), width // steps)
            parts = (wv.at[l, depth], w_v.at[l, depth, first]), (wg.at[l, depth], w_v.at[l, depth, second])
            load(("gate", l, k), w_v.at[l, depth], *parts)

    def load_halves(key, source, target):
        load(key, target, (source(mine), target.at[first]), (source(other), target.at[second]))

    head = plan.chunks[0][0] - plan.own
    load("gain", gain_v, (gain, gain_v))
    load_rows("x0", head, x_v.shape[0])
    load_gate(0, STEPS)
    load_rows("x", 0, head)
    def load_rest():
        free[:0] = range(2 + STEPS)
        load("taps", taps_v, (taps, taps_v))
        load("mats", mats_v, (mats, mats_v))
        load("bias", bias_v, (bias, bias_v))
        load("cgain", cgain_v, (cgain.at[:, mine], cgain_v.at[:, first]), (cgain.at[:, other], cgain_v.at[:, second]))
        load("cshift", cshift_v, (cshift.at[:, mine], cshift_v.at[:, first]), (cshift.at[:, other], cshift_v.at[:, second]))
        for l in range(layers):
            if l:
                load_gate(l)
            load_halves(("out", l), lambda channels: wo.at[l, channels], wo_last if l == layers - 1 else wo_v.at[l])

    fwd_v, inv_v = mats_v.at[: 2 * BLOCK], mats_v.at[2 * BLOCK : 3 * BLOCK]
    oft_v = mats_v.at[3 * BLOCK :, :BLOCK]

    for l in range(layers):
        end = plan.own + x_v.shape[0]
        gated[l, : plan.own] = jnp.zeros((plan.own, half), jnp.bfloat16)
        gated[l, end:] = jnp.zeros((plan.rows - end, half), jnp.bfloat16)

    hops = sorted({piece[1] for piece in plan.pieces})
    barrier = pltpu.get_barrier_semaphore()
    pl.semaphore_signal(barrier, inc=1, device_id={"tp": 1 - tp}, device_id_type=MESH)
    for hop in hops:
        @pl.when(sp >= hop)
        def _():
            pl.semaphore_signal(barrier, inc=1, device_id={"sp": sp - hop}, device_id_type=MESH)

    def piece_copy(l, i):
        _, hop, source, target, count = plan.pieces[i]
        return pltpu.make_async_remote_copy(
            src_ref=gated.at[l, pl.ds(source, count)],
            dst_ref=gated.at[l, pl.ds(target, count)],
            send_sem=send_sem.at[hops.index(hop)],
            recv_sem=recv_sem.at[l, plan.slots.index((hop, plan.needs[i]))],
            device_id={"sp": sp + hop},
            device_id_type=MESH,
        )

    group_of = {c: g for g, group in enumerate(plan.groups) for c in group}

    def swap_copy(l, c):
        return pltpu.make_async_remote_copy(
            src_ref=conv.at[l, own_rows(c)],
            dst_ref=peer.at[l, own_rows(c)],
            send_sem=swap_send.at[0],
            recv_sem=swap_recv.at[l, group_of[c]],
            device_id={"tp": 1 - tp},
            device_id_type=MESH,
        )

    def span(group):
        return plan.chunks[group[-1]][0], plan.chunks[group[0]][1]

    def span_rows(group):
        a, b = span(group)
        return pl.ds(a - plan.own, b - a)

    @scoped
    def gate(l, group, squares=None):
        rows = span_rows(group)
        if squares is None:
            need("gain", "x" if group[0] else "x0")
            squares = 0.0
            step = width // 4
            for k in range(0, width, step):
                x = x_v[rows, k : k + step].astype(jnp.float32)
                squares = squares + jnp.sum(x * x, axis=-1, keepdims=True)
                gained[rows, k : k + step] = (x * gain_v[l : l + 1, k : k + step]).astype(jnp.bfloat16)
        if l == 0 and ("gate", 0, STEPS - 1) not in waited:
            both = 0.0
            for k in range(STEPS):
                depth = slice(k * (width // STEPS), (k + 1) * (width // STEPS))
                need(("gate", 0, k))
                both = both + jnp.dot(gained[rows, depth], w_v[l, depth], preferred_element_type=jnp.float32)
        else:
            both = jnp.dot(gained[rows, :], w_v[l], preferred_element_type=jnp.float32)
        both = both * lax.rsqrt(squares / width + 1e-06)
        a, b = span(group)
        gated[l, a:b, :] = (both[:, :half] * jax.nn.sigmoid(both[:, half:])).astype(jnp.bfloat16)

    @scoped
    def send(l, c):
        for i, piece in enumerate(plan.pieces):
            if piece[0] == c:
                @pl.when(sp + piece[1] < plan.n_sp)
                def _():
                    piece_copy(l, i).start()

    @scoped
    def transform_taps(l):
        need("taps", "mats")
        for j in range(plan.parts):
            first = (plan.parts - 1 - j) * BLOCK
            kernels[l, j] = jnp.dot(
                oft_v[...], taps_v[l, first : first + BLOCK, :], preferred_element_type=jnp.float32
            )

    def whole(ref, sem):
        return pltpu.make_async_copy(ref, ref, sem)

    def await_group(l, g):
        for h, hop in enumerate(hops):
            spans = [(piece[3], piece[3] + piece[4]) for i, piece in enumerate(plan.pieces) if plan.needs[i] == g and piece[1] == hop]
            if spans:
                low, high = min(a for a, _ in spans), max(b for _, b in spans)
                assert high - low == sum(b - a for a, b in spans)
                with jax.named_scope(f"recv{hop}_{g}"):
                    @pl.when(sp >= hop)
                    def _():
                        whole(gated.at[l, pl.ds(low, high - low)], recv_sem.at[l, plan.slots.index((hop, g))]).wait()

    @scoped
    def spectrum(l, w):
        first, last = w * BLOCK, (w + 2) * BLOCK
        for half_bins in (slice(0, BLOCK), slice(BLOCK, 2 * BLOCK)):
            spectra[l, w, half_bins, :] = jnp.dot(
                fwd_v[half_bins, :], gated[l, first:last, :], preferred_element_type=jnp.float32
            )

    summed = {}

    def add_bins(l, c, windows, final=False):
        p = plan.outs - 1 - c
        begun = (l, c) in summed
        summed[l, c] = True
        tile = 16
        for k in range(0, BLOCK, tile):
            low, high = slice(k, k + tile), slice(BLOCK + k, BLOCK + k + tile)
            real, imag = (sums[c, low, :], sums[c, high, :]) if begun else (None, None)
            for w in windows:
                j = plan.parts - 1 + p - w
                xr, xi = spectra[l, w, low, :], spectra[l, w, high, :]
                hr, hi = kernels[l, j, low, :], kernels[l, j, high, :]
                r, i = xr * hr - xi * hi, xr * hi + xi * hr
                real, imag = (r, i) if real is None else (real + r, imag + i)
            if final:
                freq[c, low, :] = real.astype(jnp.bfloat16)
                freq[c, high, :] = imag.astype(jnp.bfloat16)
            else:
                sums[c, low, :], sums[c, high, :] = real, imag

    unused = {(l, c): [w for w in reversed(range(plan.outs - 1 - c, plan.outs - 1 - c + plan.parts))] for l in range(layers) for c in range(plan.outs)}

    def add_ready(l, c, final=False):
        ready = [w for w in unused[l, c] if (l, w) in transformed]
        unused[l, c] = [w for w in unused[l, c] if w not in ready]
        assert not (final and unused[l, c])
        if ready or final:
            add_bins(l, c, ready, final)

    def add_later(l, groups):
        for group in groups:
            for c in group:
                add_ready(l, c)

    def fence():
        pl.semaphore_signal(fence_sem, 1)
        pl.semaphore_wait(fence_sem, 1)

    def invert(l, c):
        a, b = plan.chunks[c]
        result = jnp.dot(inv_v[: b - a, :], freq[c], preferred_element_type=jnp.float32)
        conv[l, own_rows(c), :] = (result + bias_v[l : l + 1, :]).astype(jnp.bfloat16)
        swap_copy(l, c).start()

    transformed = set()

    def spectra_for(l, group, own):
        p = plan.outs - 1 - group[-1]
        q = plan.outs - 1 - group[0]
        fresh = [w for w in range(p, q + plan.parts) if (l, w) not in transformed]
        fresh = [w for w in reversed(fresh) if not own or w * BLOCK >= plan.own]
        if not own:
            await_group(l, group_of[group[0]])
        for w in fresh:
            transformed.add((l, w))
            spectrum(l, w)

    @scoped
    def convolve(l, group):
        for c in group:
            add_ready(l, c, final=True)
        for c in group:
            invert(l, c)

    def await_swap(l, group):
        with jax.named_scope("swapwait"):
            whole(peer.at[l, span_rows(group)], swap_recv.at[l, group_of[group[0]]]).wait()

    def own_mean(l, group):
        rows = span_rows(group)
        mean = jnp.mean(conv[l, rows, :].astype(jnp.float32), axis=-1, keepdims=True)
        shift[l, rows, :] = jnp.broadcast_to(mean, (mean.shape[0], LANES))

    def mix(l, group):
        rows = span_rows(group)
        need("cgain", "cshift")
        values = jnp.concatenate([conv[l, rows, :], peer[l, rows, :]], axis=-1).astype(jnp.float32)
        channels = values.shape[1]
        values = values - jnp.concatenate([shift[l, rows, :]] * (channels // LANES), axis=-1)
        center = jnp.sum(values, axis=-1, keepdims=True) / channels
        spread = jnp.sum(values * values, axis=-1, keepdims=True) / channels - center * center
        scale = lax.rsqrt(jnp.maximum(spread, 0.0) + 1e-05)
        normed = (values - center) * scale * cgain_v[l : l + 1, :] + cshift_v[l : l + 1, :]
        return (normed * jax.nn.sigmoid(normed)).astype(jnp.bfloat16)

    swapped = set()

    @scoped
    def finish(l, group, unmeaned):
        rows = span_rows(group)
        last = l == layers - 1
        for g in sorted({group_of[c] for c in group}):
            if (l, g) not in swapped:
                swapped.add((l, g))
                await_swap(l, plan.groups[g])
        for part in unmeaned:
            if group_of[part[0]] in {group_of[c] for c in group}:
                own_mean(l, part)
        need("cgain", "cshift", ("out", l))
        if not last:
            need(("gate", l + 1, 0))
        for part in unmeaned:
            if group_of[part[0]] not in {group_of[c] for c in group}:
                own_mean(l, part)
        mixed = mix(l, group)
        out = wo_last if last else wo_v.at[l]
        step = width // 4
        squares = 0.0
        for n in range(0, width, step):
            update = jnp.dot(mixed, out[:, n : n + step], preferred_element_type=jnp.float32)
            new = (x_v[rows, n : n + step].astype(jnp.float32) + update).astype(jnp.bfloat16)
            x_v[rows, n : n + step] = new
            if not last:
                x = new.astype(jnp.float32)
                squares = squares + jnp.sum(x * x, axis=-1, keepdims=True)
                gained[rows, n : n + step] = (x * gain_v[l + 1 : l + 2, n : n + step]).astype(jnp.bfloat16)
        if not last:
            gate(l + 1, group, squares)
        add_later(l, plan.groups)
        if not last:
            for c in group:
                send(l + 1, c)

    for c in range(plan.outs):
        gate(0, [c])
        if c == 0:
            load_rest()
            with jax.named_scope("barrier"):
                pl.semaphore_wait(barrier, 1 + jnp.minimum(plan.n_sp - 1 - sp, len(hops)))
        send(0, c)
    for l in range(layers):
        transform_taps(l)
    need("bias")
    for l in range(layers):
        spectra_for(l, plan.groups[0], True)
        add_later(l, plan.groups)
        unmeaned = []
        for step, which in ORDER_LAST if l == layers - 1 else ORDER:
            if step == "conv":
                group = plan.groups[which[0]]
                spectra_for(l, group, False)
                for part in unmeaned:
                    own_mean(l, part)
                convolve(l, group)
                unmeaned = [group]
                if which == [0]:
                    fence()
                    add_later(l, plan.groups[1:])
            else:
                finish(l, which, unmeaned)
                unmeaned = []

    for c in plan.tail:
        await_swap(layers - 1, [c])
        if [c] in unmeaned:
            own_mean(layers - 1, [c])
        mixed_v[own_rows(c)] = mix(layers - 1, [c])
    whole(conv, swap_send.at[0]).wait()
    for h, hop in enumerate(hops):
        count = sum(piece[4] for piece in plan.pieces if piece[1] == hop)

        @pl.when(sp + hop < plan.n_sp)
        def _():
            whole(gated.at[:, pl.ds(0, count)], send_sem.at[h]).wait()


def last_out(done, x_v, mixed, wo, result, tail, sem):
    rows, width = tail.shape
    copies = [pltpu.make_async_copy(x_v.at[a:b], result.at[a:b], sem.at[0]) for a, b in done]
    for copy in copies:
        copy.start()
    step = width // 4
    for n in range(0, width, step):
        update = jnp.dot(mixed[...], wo[:, n : n + step], preferred_element_type=jnp.float32)
        tail[:, n : n + step] = (x_v[:rows, n : n + step].astype(jnp.float32) + update).astype(jnp.bfloat16)
        copy = pltpu.make_async_copy(tail.at[:, n : n + step], result.at[:rows, n : n + step], sem.at[0])
        copy.start()
        copies.append(copy)
    for copy in copies:
        copy.wait()


def per_device(stream, norm_gain, value_weight, gate_weight, conv_taps, conv_bias, channel_gain, channel_shift, out_weight):
    tokens, width = stream.shape
    layers, reach, half = conv_taps.shape
    plan = Plan(tokens, width, reach, lax.axis_size("sp"))
    mats = dft_matrices(BLOCK)
    n_hops = len({piece[1] for piece in plan.pieces})
    bf16, f32, dma = jnp.bfloat16, jnp.float32, pltpu.SemaphoreType.DMA
    windows = plan.parts + plan.outs - 1
    last_rows = sum(b - a for a, b in (plan.chunks[c] for c in plan.tail))
    x, mixed, wo_last = pl.pallas_call(
        functools.partial(kernel, plan, layers),
        out_shape=[
            pltpu.VMEM(stream.shape, stream.dtype),
            pltpu.VMEM((last_rows, 2 * half), bf16),
            pltpu.VMEM(out_weight.shape[1:], bf16),
        ],
        in_specs=[pl.BlockSpec(memory_space=pltpu.HBM)] * 10,
        out_specs=[pl.BlockSpec(memory_space=pltpu.VMEM)] * 3,
        scratch_shapes=[
            pltpu.VMEM(norm_gain.shape, f32),
            pltpu.VMEM((layers, width, 2 * half), bf16),
            pltpu.VMEM(conv_taps.shape, bf16),
            pltpu.VMEM(conv_bias.shape, f32),
            pltpu.VMEM(channel_gain.shape, f32),
            pltpu.VMEM(channel_shift.shape, f32),
            pltpu.VMEM((layers - 1, *out_weight.shape[1:]), bf16),
            pltpu.VMEM(mats.shape, bf16),
            pltpu.VMEM((layers, plan.rows, half), bf16),
            pltpu.VMEM((tokens, width), bf16),
            pltpu.VMEM((layers, windows, 2 * BLOCK, half), f32),
            pltpu.VMEM((layers, plan.parts, 2 * BLOCK, half), f32),
            pltpu.VMEM((plan.outs, 2 * BLOCK, half), f32),
            pltpu.VMEM((plan.outs, 2 * BLOCK, half), bf16),
            pltpu.VMEM((layers, tokens, half), bf16),
            pltpu.VMEM((layers, tokens, half), bf16),
            pltpu.VMEM((layers, tokens, LANES), f32),
            dma((max(3 + STEPS, 5 + 2 * layers),)),
            dma((n_hops,)),
            dma((layers, len(plan.slots))),
            dma((1,)),
            dma((layers, len(plan.groups))),
            pltpu.SemaphoreType.REGULAR,
        ],
        compiler_params=pltpu.CompilerParams(
            collective_id=0, has_side_effects=True, vmem_limit_bytes=61300 * 1024
        ),
    )(stream, norm_gain, value_weight, gate_weight, conv_taps, conv_bias, channel_gain, channel_shift, out_weight, mats)
    done = [(plan.chunks[c][0] - plan.own, plan.chunks[c][1] - plan.own) for c in range(plan.outs) if c not in plan.tail]
    return pl.pallas_call(
        functools.partial(last_out, done),
        out_shape=jax.ShapeDtypeStruct(stream.shape, stream.dtype),
        in_specs=[pl.BlockSpec(memory_space=pltpu.VMEM)] * 3,
        out_specs=pl.BlockSpec(memory_space=pltpu.HBM),
        scratch_shapes=[pltpu.VMEM((last_rows, width), bf16), dma((1,))],
        compiler_params=pltpu.CompilerParams(vmem_limit_bytes=16000 * 1024),
    )(x, mixed, wo_last)


def solution(mesh):
    return jax.shard_map(
        per_device,
        mesh=mesh,
        in_specs=(
            P("sp", None),
            P(),
            P(None, None, "tp"),
            P(None, None, "tp"),
            P(None, None, "tp"),
            P(None, "tp"),
            P(),
            P(),
            P(),
        ),
        out_specs=P("sp", None),
        check_vma=False,
    )
```

```python
import functools

import jax
import jax.numpy as jnp
import numpy as np
from jax import lax
from jax.experimental import pallas as pl
from jax.experimental.pallas import tpu as pltpu
from jax.sharding import PartitionSpec as P

BLOCK = 128
STEPS = 4
ORDER = [("conv", [0]), ("conv", [1]), ("out", [0]), ("conv", [2]), ("out", [1]), ("conv", [3]), ("out", [2]), ("out", [3])]
ORDER_LAST = [("conv", [0]), ("conv", [1]), ("out", [0]), ("conv", [2]), ("conv", [3]), ("out", [1]), ("out", [2])]
LANES = 128
MESH = pl.DeviceIdType.MESH


def dft_matrices(block):
    span = 2 * block
    angle = 2 * np.pi / span * np.outer(np.arange(block) + 0.5, np.arange(span))
    forward = np.concatenate([np.cos(angle), -np.sin(angle)], axis=0)
    of_taps = forward[:, block - 1 :: -1]
    inverse = forward[:, block:].T / block
    of_taps = np.concatenate([of_taps, np.zeros_like(of_taps)], axis=1)
    return jnp.asarray(np.concatenate([forward, inverse, of_taps]), jnp.bfloat16)


class Plan:
    def __init__(self, tokens, width, reach, n_sp):
        self.tokens, self.n_sp = tokens, n_sp
        self.parts = reach // BLOCK
        self.outs = -(-tokens // BLOCK)
        self.rows = (self.parts + self.outs) * BLOCK
        self.own = self.parts * BLOCK
        low = self.own - reach
        self.chunks = []
        for p in reversed(range(self.outs)):
            start = (self.parts + p) * BLOCK
            self.chunks.append((start, min(start + BLOCK, self.own + tokens)))
        self.groups = [[c] for c in range(self.outs)]
        self.tail = list(range(max(self.outs - 1, 0), self.outs))
        self.pieces = []
        for c, (a, b) in enumerate(self.chunks):
            for hop in range(1, min(-(-reach // tokens), n_sp - 1) + 1):
                first, end = max(a, low + hop * tokens) - hop * tokens, b - hop * tokens
                while first < end:
                    cut = max(first, (end - 1) // BLOCK * BLOCK if hop == 1 else first)
                    when = c if hop == 1 else max(self.outs - 3, 0)
                    self.pieces.append((when, hop, cut + hop * tokens, cut, end - cut))
                    end = cut
        self.pieces.sort(key=lambda piece: piece[:2])
        self.needs = []
        for _, _, _, target, count in self.pieces:
            for g, group in enumerate(self.groups):
                if target + count > (self.outs - 1 - group[-1]) * BLOCK:
                    self.needs.append(g)
                    break
        self.slots = sorted({(piece[1], need) for piece, need in zip(self.pieces, self.needs)})


def scoped(fn):
    def named(*args):
        label = "_".join(str(a) for a in args if isinstance(a, (int, list)))
        with jax.named_scope(f"{fn.__name__}#{label}"):
            return fn(*args)

    return named


def kernel(
    plan, layers, stream, gain, wv, wg, taps, bias, cgain, cshift, wo, mats, x_v, mixed_v, wo_last,
    gain_v, w_v, taps_v, bias_v, cgain_v, cshift_v, wo_v, mats_v,
    gated, gained, spectra, kernels, sums, freq, conv, peer, shift, load_sem, send_sem, recv_sem, swap_send, swap_recv,
):
    sp, tp = lax.axis_index("sp"), lax.axis_index("tp")
    half = wv.shape[2]
    width = x_v.shape[1]
    mine = pl.ds(pl.multiple_of(tp * half, half), half)
    other = pl.ds(pl.multiple_of((1 - tp) * half, half), half)
    first, second = pl.ds(0, half), pl.ds(half, half)
    loads = {}
    free = list(range(load_sem.shape[0]))
    waited = set()

    def load(key, whole, *parts):
        sem = load_sem.at[free.pop(0)]
        loads[key] = pltpu.make_async_copy(whole, whole, sem)
        for source, target in parts:
            pltpu.make_async_copy(source, target, sem).start()

    def need(*keys):
        for key in keys:
            if key not in waited:
                waited.add(key)
                loads[key].wait()

    def own_rows(c):
        a, b = plan.chunks[c]
        return pl.ds(a - plan.own, b - a)

    def load_rows(key, a, b):
        rows = pl.ds(a, b - a)
        load(key, x_v.at[rows], (stream.at[rows], x_v.at[rows]))

    def load_gate(l, steps=1):
        for k in range(steps):
            depth = pl.ds(k * (width // steps), width // steps)
            parts = (wv.at[l, depth], w_v.at[l, depth, first]), (wg.at[l, depth], w_v.at[l, depth, second])
            load(("gate", l, k), w_v.at[l, depth], *parts)

    def load_halves(key, source, target):
        load(key, target, (source(mine), target.at[first]), (source(other), target.at[second]))

    head = plan.chunks[0][0] - plan.own
    load("gain", gain_v, (gain, gain_v))
    load_rows("x0", head, x_v.shape[0])
    load_gate(0, STEPS)
    load_rows("x", 0, head)
    def load_rest():
        free[:0] = range(2 + STEPS)
        load("taps", taps_v, (taps, taps_v))
        load("mats", mats_v, (mats, mats_v))
        load("bias", bias_v, (bias, bias_v))
        load("cgain", cgain_v, (cgain.at[:, mine], cgain_v.at[:, first]), (cgain.at[:, other], cgain_v.at[:, second]))
        load("cshift", cshift_v, (cshift.at[:, mine], cshift_v.at[:, first]), (cshift.at[:, other], cshift_v.at[:, second]))
        for l in range(layers):
            if l:
                load_gate(l)
            load_halves(("out", l), lambda channels: wo.at[l, channels], wo_last if l == layers - 1 else wo_v.at[l])

    fwd_v, inv_v = mats_v.at[: 2 * BLOCK], mats_v.at[2 * BLOCK : 3 * BLOCK]
    oft_v = mats_v.at[3 * BLOCK :, :BLOCK]

    for l in range(layers):
        end = plan.own + x_v.shape[0]
        gated[l, : plan.own] = jnp.zeros((plan.own, half), jnp.bfloat16)
        gated[l, end:] = jnp.zeros((plan.rows - end, half), jnp.bfloat16)

    hops = sorted({piece[1] for piece in plan.pieces})
    barrier = pltpu.get_barrier_semaphore()
    pl.semaphore_signal(barrier, inc=1, device_id={"tp": 1 - tp}, device_id_type=MESH)
    for hop in hops:
        @pl.when(sp >= hop)
        def _():
            pl.semaphore_signal(barrier, inc=1, device_id={"sp": sp - hop}, device_id_type=MESH)

    def piece_copy(l, i):
        _, hop, source, target, count = plan.pieces[i]
        return pltpu.make_async_remote_copy(
            src_ref=gated.at[l, pl.ds(source, count)],
            dst_ref=gated.at[l, pl.ds(target, count)],
            send_sem=send_sem.at[hops.index(hop)],
            recv_sem=recv_sem.at[l, plan.slots.index((hop, plan.needs[i]))],
            device_id={"sp": sp + hop},
            device_id_type=MESH,
        )

    group_of = {c: g for g, group in enumerate(plan.groups) for c in group}

    def swap_copy(l, c):
        return pltpu.make_async_remote_copy(
            src_ref=conv.at[l, own_rows(c)],
            dst_ref=peer.at[l, own_rows(c)],
            send_sem=swap_send.at[0],
            recv_sem=swap_recv.at[l, group_of[c]],
            device_id={"tp": 1 - tp},
            device_id_type=MESH,
        )

    def span(group):
        return plan.chunks[group[-1]][0], plan.chunks[group[0]][1]

    def span_rows(group):
        a, b = span(group)
        return pl.ds(a - plan.own, b - a)

    @scoped
    def gate(l, group, squares=None):
        rows = span_rows(group)
        if squares is None:
            need("gain", "x" if group[0] else "x0")
            squares = 0.0
            step = width // 4
            for k in range(0, width, step):
                x = x_v[rows, k : k + step].astype(jnp.float32)
                squares = squares + jnp.sum(x * x, axis=-1, keepdims=True)
                gained[rows, k : k + step] = (x * gain_v[l : l + 1, k : k + step]).astype(jnp.bfloat16)
        if l == 0 and ("gate", 0, STEPS - 1) not in waited:
            both = 0.0
            for k in range(STEPS):
                depth = slice(k * (width // STEPS), (k + 1) * (width // STEPS))
                need(("gate", 0, k))
                both = both + jnp.dot(gained[rows, depth], w_v[l, depth], preferred_element_type=jnp.float32)
        else:
            both = jnp.dot(gained[rows, :], w_v[l], preferred_element_type=jnp.float32)
        both = both * lax.rsqrt(squares / width + 1e-06)
        a, b = span(group)
        gated[l, a:b, :] = (both[:, :half] * jax.nn.sigmoid(both[:, half:])).astype(jnp.bfloat16)

    @scoped
    def send(l, c):
        for i, piece in enumerate(plan.pieces):
            if piece[0] == c:
                @pl.when(sp + piece[1] < plan.n_sp)
                def _():
                    piece_copy(l, i).start()

    @scoped
    def transform_taps(l):
        need("taps", "mats")
        for j in range(plan.parts):
            first = (plan.parts - 1 - j) * BLOCK
            kernels[l, j] = jnp.dot(
                oft_v[...], taps_v[l, first : first + BLOCK, :], preferred_element_type=jnp.float32
            )

    def whole(ref, sem):
        return pltpu.make_async_copy(ref, ref, sem)

    def await_group(l, g):
        for h, hop in enumerate(hops):
            spans = [(piece[3], piece[3] + piece[4]) for i, piece in enumerate(plan.pieces) if plan.needs[i] == g and piece[1] == hop]
            if spans:
                low, high = min(a for a, _ in spans), max(b for _, b in spans)
                assert high - low == sum(b - a for a, b in spans)
                with jax.named_scope(f"recv{hop}_{g}"):
                    @pl.when(sp >= hop)
                    def _():
                        whole(gated.at[l, pl.ds(low, high - low)], recv_sem.at[l, plan.slots.index((hop, g))]).wait()

    @scoped
    def spectrum(l, w):
        first, last = w * BLOCK, (w + 2) * BLOCK
        for half_bins in (slice(0, BLOCK), slice(BLOCK, 2 * BLOCK)):
            spectra[l, w, half_bins, :] = jnp.dot(
                fwd_v[half_bins, :], gated[l, first:last, :], preferred_element_type=jnp.float32
            )

    summed = {}

    def add_bins(l, c, windows, final=False):
        p = plan.outs - 1 - c
        begun = (l, c) in summed
        summed[l, c] = True
        tile = 16
        for k in range(0, BLOCK, tile):
            low, high = slice(k, k + tile), slice(BLOCK + k, BLOCK + k + tile)
            real, imag = (sums[c, low, :], sums[c, high, :]) if begun else (None, None)
            for w in windows:
                j = plan.parts - 1 + p - w
                xr, xi = spectra[l, w, low, :], spectra[l, w, high, :]
                hr, hi = kernels[l, j, low, :], kernels[l, j, high, :]
                r, i = xr * hr - xi * hi, xr * hi + xi * hr
                real, imag = (r, i) if real is None else (real + r, imag + i)
            if final:
                freq[c, low, :] = real.astype(jnp.bfloat16)
                freq[c, high, :] = imag.astype(jnp.bfloat16)
            else:
                sums[c, low, :], sums[c, high, :] = real, imag

    unused = {(l, c): [w for w in reversed(range(plan.outs - 1 - c, plan.outs - 1 - c + plan.parts))] for l in range(layers) for c in range(plan.outs)}

    def add_ready(l, c, final=False):
        ready = [w for w in unused[l, c] if (l, w) in transformed]
        unused[l, c] = [w for w in unused[l, c] if w not in ready]
        assert not (final and unused[l, c])
        if ready or final:
            add_bins(l, c, ready, final)

    def add_later(l, groups):
        for group in groups:
            for c in group:
                add_ready(l, c)

    def invert(l, c):
        a, b = plan.chunks[c]
        result = jnp.dot(inv_v[: b - a, :], freq[c], preferred_element_type=jnp.float32)
        conv[l, own_rows(c), :] = (result + bias_v[l : l + 1, :]).astype(jnp.bfloat16)
        swap_copy(l, c).start()

    transformed = set()

    def spectra_for(l, group, own):
        p = plan.outs - 1 - group[-1]
        q = plan.outs - 1 - group[0]
        fresh = [w for w in range(p, q + plan.parts) if (l, w) not in transformed]
        fresh = [w for w in reversed(fresh) if not own or w * BLOCK >= plan.own]
        if not own:
            await_group(l, group_of[group[0]])
        for w in fresh:
            transformed.add((l, w))
            spectrum(l, w)

    @scoped
    def convolve(l, group):
        for c in group:
            add_ready(l, c, final=True)
        for c in group:
            invert(l, c)

    def await_swap(l, group):
        with jax.named_scope("swapwait"):
            whole(peer.at[l, span_rows(group)], swap_recv.at[l, group_of[group[0]]]).wait()

    def own_mean(l, group):
        rows = span_rows(group)
        mean = jnp.mean(conv[l, rows, :].astype(jnp.float32), axis=-1, keepdims=True)
        shift[l, rows, :] = jnp.broadcast_to(mean, (mean.shape[0], LANES))

    def mix(l, group):
        rows = span_rows(group)
        need("cgain", "cshift")
        values = jnp.concatenate([conv[l, rows, :], peer[l, rows, :]], axis=-1).astype(jnp.float32)
        channels = values.shape[1]
        values = values - jnp.concatenate([shift[l, rows, :]] * (channels // LANES), axis=-1)
        center = jnp.sum(values, axis=-1, keepdims=True) / channels
        spread = jnp.sum(values * values, axis=-1, keepdims=True) / channels - center * center
        scale = lax.rsqrt(jnp.maximum(spread, 0.0) + 1e-05)
        normed = (values - center) * scale * cgain_v[l : l + 1, :] + cshift_v[l : l + 1, :]
        return (normed * jax.nn.sigmoid(normed)).astype(jnp.bfloat16)

    swapped = set()

    @scoped
    def finish(l, group, unmeaned):
        rows = span_rows(group)
        last = l == layers - 1
        for g in sorted({group_of[c] for c in group}):
            if (l, g) not in swapped:
                swapped.add((l, g))
                await_swap(l, plan.groups[g])
        for part in unmeaned:
            if group_of[part[0]] in {group_of[c] for c in group}:
                own_mean(l, part)
        need("cgain", "cshift", ("out", l))
        if not last:
            need(("gate", l + 1, 0))
        for part in unmeaned:
            if group_of[part[0]] not in {group_of[c] for c in group}:
                own_mean(l, part)
        mixed = mix(l, group)
        out = wo_last if last else wo_v.at[l]
        step = width // 4
        squares = 0.0
        for n in range(0, width, step):
            update = jnp.dot(mixed, out[:, n : n + step], preferred_element_type=jnp.float32)
            x = x_v[rows, n : n + step].astype(jnp.float32) + update
            x_v[rows, n : n + step] = x.astype(jnp.bfloat16)
            if not last:
                squares = squares + jnp.sum(x * x, axis=-1, keepdims=True)
                gained[rows, n : n + step] = (x * gain_v[l + 1 : l + 2, n : n + step]).astype(jnp.bfloat16)
        if not last:
            gate(l + 1, group, squares)
        add_later(l, plan.groups)
        if not last:
            for c in group:
                send(l + 1, c)

    for c in range(plan.outs):
        gate(0, [c])
        if c == 0:
            load_rest()
            with jax.named_scope("barrier"):
                pl.semaphore_wait(barrier, 1 + jnp.minimum(plan.n_sp - 1 - sp, len(hops)))
        send(0, c)
    for l in range(layers):
        transform_taps(l)
    need("bias")
    for l in range(layers):
        spectra_for(l, plan.groups[0], True)
        add_later(l, plan.groups)
        unmeaned = []
        for step, which in ORDER_LAST if l == layers - 1 else ORDER:
            if step == "conv":
                group = plan.groups[which[0]]
                spectra_for(l, group, False)
                for part in unmeaned:
                    own_mean(l, part)
                convolve(l, group)
                unmeaned = [group]
                if which == [0]:
                    add_later(l, plan.groups[1:])
            else:
                finish(l, which, unmeaned)
                unmeaned = []

    for c in plan.tail:
        await_swap(layers - 1, [c])
        if [c] in unmeaned:
            own_mean(layers - 1, [c])
        mixed_v[own_rows(c)] = mix(layers - 1, [c])
    whole(conv, swap_send.at[0]).wait()
    for h, hop in enumerate(hops):
        count = sum(piece[4] for piece in plan.pieces if piece[1] == hop)

        @pl.when(sp + hop < plan.n_sp)
        def _():
            whole(gated.at[:, pl.ds(0, count)], send_sem.at[h]).wait()


def last_out(done, x_v, mixed, wo, result, tail, sem):
    rows, width = tail.shape
    copies = [pltpu.make_async_copy(x_v.at[a:b], result.at[a:b], sem.at[0]) for a, b in done]
    for copy in copies:
        copy.start()
    step = width // 4
    for n in range(0, width, step):
        update = jnp.dot(mixed[...], wo[:, n : n + step], preferred_element_type=jnp.float32)
        tail[:, n : n + step] = (x_v[:rows, n : n + step].astype(jnp.float32) + update).astype(jnp.bfloat16)
        copy = pltpu.make_async_copy(tail.at[:, n : n + step], result.at[:rows, n : n + step], sem.at[0])
        copy.start()
        copies.append(copy)
    for copy in copies:
        copy.wait()


def per_device(stream, norm_gain, value_weight, gate_weight, conv_taps, conv_bias, channel_gain, channel_shift, out_weight):
    tokens, width = stream.shape
    layers, reach, half = conv_taps.shape
    plan = Plan(tokens, width, reach, lax.axis_size("sp"))
    mats = dft_matrices(BLOCK)
    n_hops = len({piece[1] for piece in plan.pieces})
    bf16, f32, dma = jnp.bfloat16, jnp.float32, pltpu.SemaphoreType.DMA
    windows = plan.parts + plan.outs - 1
    last_rows = sum(b - a for a, b in (plan.chunks[c] for c in plan.tail))
    x, mixed, wo_last = pl.pallas_call(
        functools.partial(kernel, plan, layers),
        out_shape=[
            pltpu.VMEM(stream.shape, stream.dtype),
            pltpu.VMEM((last_rows, 2 * half), bf16),
            pltpu.VMEM(out_weight.shape[1:], bf16),
        ],
        in_specs=[pl.BlockSpec(memory_space=pltpu.HBM)] * 10,
        out_specs=[pl.BlockSpec(memory_space=pltpu.VMEM)] * 3,
        scratch_shapes=[
            pltpu.VMEM(norm_gain.shape, f32),
            pltpu.VMEM((layers, width, 2 * half), bf16),
            pltpu.VMEM(conv_taps.shape, bf16),
            pltpu.VMEM(conv_bias.shape, f32),
            pltpu.VMEM(channel_gain.shape, f32),
            pltpu.VMEM(channel_shift.shape, f32),
            pltpu.VMEM((layers - 1, *out_weight.shape[1:]), bf16),
            pltpu.VMEM(mats.shape, bf16),
            pltpu.VMEM((layers, plan.rows, half), bf16),
            pltpu.VMEM((tokens, width), bf16),
            pltpu.VMEM((layers, windows, 2 * BLOCK, half), f32),
            pltpu.VMEM((layers, plan.parts, 2 * BLOCK, half), f32),
            pltpu.VMEM((plan.outs, 2 * BLOCK, half), f32),
            pltpu.VMEM((plan.outs, 2 * BLOCK, half), bf16),
            pltpu.VMEM((layers, tokens, half), bf16),
            pltpu.VMEM((layers, tokens, half), bf16),
            pltpu.VMEM((layers, tokens, LANES), f32),
            dma((max(3 + STEPS, 5 + 2 * layers),)),
            dma((n_hops,)),
            dma((layers, len(plan.slots))),
            dma((1,)),
            dma((layers, len(plan.groups))),
        ],
        compiler_params=pltpu.CompilerParams(
            collective_id=0, has_side_effects=True, vmem_limit_bytes=61300 * 1024
        ),
    )(stream, norm_gain, value_weight, gate_weight, conv_taps, conv_bias, channel_gain, channel_shift, out_weight, mats)
    done = [(plan.chunks[c][0] - plan.own, plan.chunks[c][1] - plan.own) for c in range(plan.outs) if c not in plan.tail]
    return pl.pallas_call(
        functools.partial(last_out, done),
        out_shape=jax.ShapeDtypeStruct(stream.shape, stream.dtype),
        in_specs=[pl.BlockSpec(memory_space=pltpu.VMEM)] * 3,
        out_specs=pl.BlockSpec(memory_space=pltpu.HBM),
        scratch_shapes=[pltpu.VMEM((last_rows, width), bf16), dma((1,))],
        compiler_params=pltpu.CompilerParams(vmem_limit_bytes=16000 * 1024),
    )(x, mixed, wo_last)


def solution(mesh):
    return jax.shard_map(
        per_device,
        mesh=mesh,
        in_specs=(
            P("sp", None),
            P(),
            P(None, None, "tp"),
            P(None, None, "tp"),
            P(None, None, "tp"),
            P(None, "tp"),
            P(),
            P(),
            P(),
        ),
        out_specs=P("sp", None),
        check_vma=False,
    )
```
